768 devices in a mesh: ep: 48 (over z, x), tp: 16 (over y, core).
Axes of the slice: x: 4, y: 8, z: 12, core: 2. Of those that a mesh axis runs over, the one named last changes fastest.
Arguments:
- tokens: bfloat16 [147456, 2048], P(('ep', 'tp')), may hold values from -6 to 6
- routes: int32 [147456, 2], P(('ep', 'tp')), may hold values from 0 to 47, all different within a row; in each aligned block of 192 rows (0 to 191, 192 to 383, ...) at most 10 rows name the same one
- gates: float32 [147456, 2], P(('ep', 'tp')), may hold values from 0.3 to 2.2
- pre_gain: float32 [2048], replicated, may hold values from 0.1 to 1.9
- w_gate: bfloat16 [48, 2048, 512], P('ep'), may hold values from -0.125 to 0.125
- w_up: bfloat16 [48, 2048, 512], P('ep'), may hold values from -0.125 to 0.125
- w_down: bfloat16 [48, 512, 2048], P('ep'), may hold values from -0.25 to 0.25
- sh_gate: bfloat16 [2048, 512], P('tp'), may hold values from -0.125 to 0.125
- sh_up: bfloat16 [2048, 512], P('tp'), may hold values from -0.125 to 0.125
- sh_down: bfloat16 [512, 2048], P(None, 'tp'), may hold values from -0.25 to 0.25
- post_gain: float32 [2048], replicated, may hold values from 0.1 to 1.9
Outputs:
- mixed: bfloat16 [147456, 2048], P('ep', 'tp')
The draws below stay inside these ranges and needn't reach their ends.
Inputs may be any that keep to these rules, and one draw needn't show every extreme that they name: `routes`: each token names 2 different experts; among the rows of one device no expert is named more than 10 times, a bound that some block reaches.
All inputs are finite; a program needn't handle non-finite values.
Results may differ from the reference program's by a relative error of at most 0.0075.
Values may be sent and summed in bfloat16 or wider, within the bound.
A program may use at most 64 MiB of HBM per device.

```python
import math
import jax
import jax.numpy as jnp
import numpy as np
from jax import lax

D = 2048
FF = 512
SH = 512
TOPK = 2
TOK_DEV = 192
EXPERTS = 48
CAP = 10
TOKENS = 147456
N_EP = 48
N_TP = 16


def levels(key, shape, shards, smallest, largest):
    def one(axis_at, parts):
        draws = jax.random.uniform(jax.random.fold_in(jax.random.fold_in(key, 6), axis_at), (parts,), jnp.float32, smallest / len(shards), largest / len(shards))
        return jnp.repeat(jnp.exp(draws), shape[axis_at] // parts).reshape((-1,) + (1,) * (len(shape) - axis_at - 1))

    factor_of = one(*shards[0])
    for cut in shards[1:]:
        factor_of = factor_of * one(*cut)
    return factor_of


def assign_block(stream_key, own, number, rows, amount, top, limit, skew):
    ranking = jax.random.permutation(stream_key, amount)
    crowded, ordinary = portions_of(amount, rows * top, limit, skew, True), portions_of(amount, rows * top, limit, skew, False)
    places = jnp.arange(amount)

    def named(lengths, turn):
        used = int((lengths > 0).sum())
        fixed = max(1, used // 4)
        passed = fixed + (places - fixed + turn * (used - fixed)) % max(1, amount - fixed)
        return jnp.zeros((amount,), jnp.int32).at[ranking[jnp.where(places < fixed, places, passed)]].set(jnp.asarray(lengths, jnp.int32))

    lengths = jnp.where(number % 4 == 0, named(crowded, number // 4), named(ordinary, number - number // 4 - 1))
    mixed = jax.random.permutation(jax.random.fold_in(own, 3), amount)
    source_of, taker = mixed[0:amount // 2 * 2:2], mixed[1:amount // 2 * 2:2]
    margin = jnp.minimum(lengths[source_of] - 1, limit - lengths[taker]) // 2
    margin = jnp.where((source_of == ranking[0]) | (taker == ranking[0]) | (lengths[taker] == 0), 0, jnp.maximum(margin, 0))
    passed = jax.random.randint(jax.random.fold_in(own, 4), (amount // 2,), 0, 1 << 20) % (margin + 1)
    lengths = lengths.at[source_of].add(-passed).at[taker].add(passed)
    members = jnp.searchsorted(jnp.cumsum(lengths), jnp.arange(rows * top), side="right").astype(jnp.int32)
    grid = members.reshape(top, rows).T
    grid = grid[jax.random.permutation(jax.random.fold_in(own, 1), rows)]
    turn = jax.random.randint(jax.random.fold_in(own, 2), (rows, 1), 0, top)
    return jnp.take_along_axis(grid, (jnp.arange(top)[None, :] + turn) % top, axis=1)


def portions_of(count, total, limit, slope, full):
    portions = [(1 << 20) // math.isqrt(standing ** slope) + 1 for standing in range(1, count + 1)]
    largest = limit if full else min(limit, max(-(-total // count), total * portions[0] // sum(portions)))
    least = 1 if total - largest >= count - 1 else 0
    counts, spare = [largest] + [least] * (count - 1), total - largest - least * (count - 1)
    while spare > 0:
        free = [i for i in range(1, count) if counts[i] < largest] or [i for i in range(1, count) if counts[i] < limit]
        mass, remaining = sum([portions[i] for i in free]), spare
        for i in free:
            addition = min(limit - counts[i], max(1, remaining * portions[i] // mass), spare)
            counts[i] = counts[i] + addition
            spare = spare - addition
    return np.array(counts)


def normal_values(key, shape, scale, reach, split=(), kind=jnp.bfloat16):
    drawn = jax.random.normal(key, shape, jnp.float32) * scale
    if len(split) > 0:
        drawn = levels(key, shape, split, -0.22, 0.18) * drawn
    return jnp.clip(drawn, min=-reach, max=reach).astype(kind)


def setup_inputs(seed: int = 0) -> dict:
    key_of = jax.random.split(jax.random.key(seed), 12)
    tokens = normal_values(key_of[0], (TOKENS, D), 1.0, 6.0, ((0, 768),))
    routes_keys = jax.random.split(jax.random.fold_in(key_of[1], 1), TOKENS // TOK_DEV)
    routes_turns = jax.random.permutation(jax.random.fold_in(key_of[1], 3), TOKENS // TOK_DEV)
    routes = jax.vmap(lambda own, number: assign_block(jax.random.fold_in(key_of[1], 2), own, number, TOK_DEV, EXPERTS, TOPK, CAP, 2))(routes_keys, routes_turns).reshape((TOKENS, TOPK))
    gates = jnp.clip(0.3 + 1.90000004 * jax.random.uniform(key_of[2], (TOKENS, TOPK), jnp.float32) ** levels(key_of[2], (TOKENS, TOPK), ((0, 768),), -0.2, 0.2), 0.3, 2.2)
    pre_gain = jnp.clip(1.0 + 0.18 * jax.random.normal(key_of[3], (D,), jnp.float32), 0.1, 1.9)
    w_gate = normal_values(key_of[4], (EXPERTS, D, FF), D ** -0.5, 0.125, ((0, 48),))
    w_up = normal_values(key_of[5], (EXPERTS, D, FF), D ** -0.5, 0.125, ((0, 48),))
    w_down = normal_values(key_of[6], (EXPERTS, FF, D), FF ** -0.5, 0.25, ((0, 48),))
    sh_gate = normal_values(key_of[7], (D, SH), D ** -0.5, 0.125, ((0, 16),))
    sh_up = normal_values(key_of[8], (D, SH), D ** -0.5, 0.125, ((0, 16),))
    sh_down = normal_values(key_of[9], (SH, D), SH ** -0.5, 0.25, ((1, 16),))
    post_gain = jnp.clip(1.0 + 0.18 * jax.random.normal(key_of[10], (D,), jnp.float32), 0.1, 1.9)
    return dict(tokens=tokens, routes=routes, gates=gates, pre_gain=pre_gain, w_gate=w_gate, w_up=w_up, w_down=w_down, sh_gate=sh_gate, sh_up=sh_up, sh_down=sh_down, post_gain=post_gain)


def rms_scale(values):
    return lax.rsqrt(lax.optimization_barrier(jnp.mean(values * values, axis=-1, keepdims=True)) + 1e-06)

def reference(tokens, routes, gates, pre_gain, w_gate, w_up, w_down, sh_gate, sh_up, sh_down, post_gain):
    devices_all = N_EP * N_TP
    per_device = TOK_DEV * TOPK
    inputs = tokens.astype(jnp.float32)
    normed = (inputs * rms_scale(inputs) * pre_gain.astype(jnp.float32)).astype(jnp.bfloat16)
    expert_ids = routes.reshape(devices_all, per_device).astype(jnp.int32)
    matches = (expert_ids[:, :, None] == jnp.arange(EXPERTS, dtype=jnp.int32)[None, None, :]).astype(jnp.int32)
    earlier = jnp.cumsum(matches, axis=1) - matches
    slot_index = lax.optimization_barrier(jnp.sum(earlier * matches, axis=2)).astype(jnp.int32)
    sources = jnp.broadcast_to(jnp.arange(devices_all, dtype=jnp.int32)[:, None], (devices_all, per_device))
    token_index = sources * TOK_DEV + jnp.arange(per_device, dtype=jnp.int32)[None, :] // TOPK
    table = jnp.full((EXPERTS, devices_all, CAP), TOKENS, jnp.int32).at[expert_ids, sources, slot_index].set(token_index)
    weight_table = jnp.zeros((EXPERTS, devices_all, CAP), jnp.float32).at[expert_ids, sources, slot_index].set(gates.reshape(devices_all, per_device).astype(jnp.float32))
    padded = jnp.concatenate([normed, jnp.zeros((1, D), jnp.bfloat16)], axis=0)

    def one_expert(summed, pack):
        rows_index, row_weight, gate_mat, up_mat, down_mat = pack
        picked = padded[rows_index]
        gate_part = jnp.dot(picked, gate_mat, preferred_element_type=jnp.float32)
        up_part = jnp.dot(picked, up_mat, preferred_element_type=jnp.float32)
        hidden = (jax.nn.silu(gate_part) * up_part).astype(jnp.bfloat16)
        result = jnp.dot(hidden, down_mat, preferred_element_type=jnp.float32).astype(jnp.bfloat16)
        summed = summed.at[rows_index].add(row_weight[:, None] * result.astype(jnp.float32))
        return (summed, None)
    summed, _ = lax.scan(one_expert, jnp.zeros((TOKENS + 1, D), jnp.float32), (table.reshape(EXPERTS, -1), weight_table.reshape(EXPERTS, -1), w_gate, w_up, w_down))
    routed = summed[:TOKENS].astype(jnp.bfloat16)
    gate_shared = jnp.dot(normed, sh_gate, preferred_element_type=jnp.float32)
    up_shared = jnp.dot(normed, sh_up, preferred_element_type=jnp.float32)
    shared_hidden = (jax.nn.silu(gate_shared) * up_shared).astype(jnp.bfloat16)
    shared = jnp.dot(shared_hidden, sh_down, preferred_element_type=jnp.float32).astype(jnp.bfloat16)
    combined = routed.astype(jnp.float32) + shared.astype(jnp.float32)
    return (combined * rms_scale(combined) * post_gain.astype(jnp.float32)).astype(jnp.bfloat16)
```

```python
import jax
import jax.numpy as jnp
from jax import lax
from jax.sharding import PartitionSpec as P

TOPK = 2


def per_device(
    tokens, routes, gates, pre_gain, w_gate, w_up, w_down, sh_gate, sh_up, sh_down, post_gain
):
    tok_rows, full_width = tokens.shape
    experts_all = lax.axis_size("ep")
    capacity = max(2, 4 * tok_rows * TOPK // (3 * experts_all))
    inputs = tokens.astype(jnp.float32)
    scale_in = lax.rsqrt(jnp.mean(inputs * inputs, axis=1, keepdims=True) + 1e-06)
    normed = (inputs * scale_in * pre_gain[None, :]).astype(jnp.bfloat16)
    gate_shared = jnp.dot(
        normed,
        lax.all_gather(sh_gate, "tp", axis=0, tiled=True),
        preferred_element_type=jnp.float32,
    )
    up_shared = jnp.dot(
        normed, lax.all_gather(sh_up, "tp", axis=0, tiled=True), preferred_element_type=jnp.float32
    )
    shared_hidden = (jax.nn.silu(gate_shared) * up_shared).astype(jnp.bfloat16)
    pair_count = tok_rows * TOPK
    expert_ids = routes.reshape(pair_count)
    matches = (expert_ids[:, None] == jnp.arange(experts_all, dtype=jnp.int32)[None, :]).astype(
        jnp.int32
    )
    earlier = jnp.cumsum(matches, axis=0) - matches
    slot_index = jnp.sum(earlier * matches, axis=1)
    dest_slot = expert_ids * capacity + slot_index
    pair_token = jnp.arange(pair_count, dtype=jnp.int32) // TOPK
    slot_token = (
        jnp.full((experts_all * capacity,), tok_rows, jnp.int32).at[dest_slot].set(pair_token)
    )
    padded = jnp.concatenate([normed, jnp.zeros((1, full_width), jnp.bfloat16)], axis=0)
    lanes = 128
    subrows = capacity * full_width // lanes
    outgoing = padded[slot_token].reshape(experts_all, subrows, lanes)
    arrived = lax.all_to_all(outgoing, "ep", split_axis=0, concat_axis=0, tiled=True)
    flat_rows = arrived.reshape(experts_all * capacity, full_width)
    gate_part = jnp.dot(flat_rows, w_gate[0], preferred_element_type=jnp.float32)
    up_part = jnp.dot(flat_rows, w_up[0], preferred_element_type=jnp.float32)
    hidden = (jax.nn.silu(gate_part) * up_part).astype(jnp.bfloat16)
    result = jnp.dot(hidden, w_down[0], preferred_element_type=jnp.float32).astype(jnp.bfloat16)
    returned = lax.all_to_all(
        result.reshape(experts_all, subrows, lanes), "ep", split_axis=0, concat_axis=0, tiled=True
    )
    picked = returned.reshape(experts_all * capacity, full_width)[dest_slot]
    weighted = picked.astype(jnp.float32) * gates.reshape(pair_count)[:, None]
    routed = jnp.sum(weighted.reshape(tok_rows, TOPK, full_width), axis=1).astype(jnp.bfloat16)
    shared = jnp.dot(
        shared_hidden,
        lax.all_gather(sh_down, "tp", axis=1, tiled=True),
        preferred_element_type=jnp.float32,
    ).astype(jnp.bfloat16)
    combined = routed.astype(jnp.float32) + shared.astype(jnp.float32)
    scale_out = lax.rsqrt(jnp.mean(combined * combined, axis=1, keepdims=True) + 1e-06)
    out_rows = (combined * scale_out * post_gain[None, :]).astype(jnp.bfloat16)
    return lax.all_to_all(out_rows, "tp", split_axis=1, concat_axis=0, tiled=True)


def solution(mesh):
    return jax.shard_map(
        per_device,
        mesh=mesh,
        in_specs=(
            P(("ep", "tp"), None),
            P(("ep", "tp"), None),
            P(("ep", "tp"), None),
            P(),
            P("ep", None, None),
            P("ep", None, None),
            P("ep", None, None),
            P("tp", None),
            P("tp", None),
            P(None, "tp"),
            P(),
        ),
        out_specs=P("ep", "tp"),
        check_vma=False,
    )
```

```python
import functools

import jax
import jax.numpy as jnp
from jax import lax
from jax.experimental import pallas as pl
from jax.experimental.pallas import tpu as pltpu
from jax.sharding import PartitionSpec as P

TOPK = 2
LANES = 128
TILE = 16
MESH = pl.DeviceIdType.MESH
F32 = jnp.float32
BF16 = jnp.bfloat16


def dot(a, b):
    return jnp.dot(a, b, preferred_element_type=F32)


def silu_mul(gate, up):
    return (gate / (1.0 + jnp.exp(-gate)) * up).astype(BF16)


def offset_at(place, n_ep):
    near = n_ep - 1 - place
    odd = lax.rem(near, 2)
    return odd * ((near + 1) // 2) + (1 - odd) * (n_ep - near // 2)


def rows_to_tiles(swap, read, width):
    stacked = jnp.concatenate(
        [read(pl.ds(LANES * j, LANES)) for j in range(width // LANES)], axis=0
    )
    return dot(swap, stacked).astype(BF16).reshape(TILE, TILE, LANES)


def tiles_to_rows(swap, tiles, write):
    flat = dot(swap, tiles.reshape(TILE * TILE, LANES)).astype(BF16)
    for j in range(TILE):
        write(pl.ds(LANES * j, LANES), flat[TILE * j : TILE * (j + 1), :])


def kernel(
    n_ep, n_tp, cap, chunk,
    tokens, routes, gates, pre_gain, w_gate, w_up, w_down, sh_gate, sh_up, sh_down, post_gain,
    out,
    normed, pick, swap, flat, outgoing, arrived, results, returned,
    wg, wu, wd, xs, rs, all_gate, all_up, all_down, shared, combined, out_blocks, out_landed,
    w_sem, send_sem, arrive_sem, back_send, back_recv,
    sh_send, sh_recv, pair_send, pair_recv, out_send, out_recv, last_sem,
):
    me, tp = lax.axis_index("ep"), lax.axis_index("tp")
    core, row = lax.rem(tp, 2), tp // 2
    n_row = n_tp // 2
    rows, width = tokens.shape
    slots = n_ep * cap
    n_chunks = n_ep // chunk
    span = chunk * cap
    out_width = width // n_tp

    barrier = pltpu.get_barrier_semaphore()

    def greet_ep(i, carry):
        pl.semaphore_signal(
            barrier, inc=1, device_id=(lax.rem(me + i, n_ep), tp), device_id_type=MESH
        )
        return carry

    def greet_tp(i, carry):
        pl.semaphore_signal(
            barrier, inc=1, device_id=(me, lax.rem(tp + i, n_tp)), device_id_type=MESH
        )
        return carry

    lax.fori_loop(1, n_ep, greet_ep, 0)
    lax.fori_loop(1, n_tp, greet_tp, 0)

    weight_copies = [
        pltpu.make_async_copy(source, target, w_sem.at[i])
        for i, (source, target) in enumerate(((w_gate, wg), (w_up, wu), (w_down, wd)))
    ]
    for copy in weight_copies:
        copy.start()

    def norm_rows(i, carry):
        at = pl.ds(pl.multiple_of(i * TILE, TILE), TILE)
        values = tokens[at, :].astype(F32)
        scale = lax.rsqrt(jnp.mean(values * values, axis=1, keepdims=True) + 1e-06)
        normed[at, :] = (values * scale * pre_gain[...]).astype(BF16)
        return carry

    lax.fori_loop(0, rows // TILE, norm_rows, 0)

    expert = lax.broadcasted_iota(jnp.int32, (rows, LANES), 1)
    first, second = routes[:, 0:1], routes[:, 1:2]
    match0 = jnp.where(first == expert, 1.0, 0.0).astype(F32)
    match1 = jnp.where(second == expert, 1.0, 0.0).astype(F32)
    earlier = jnp.where(
        lax.broadcasted_iota(jnp.int32, (rows, rows), 1)
        < lax.broadcasted_iota(jnp.int32, (rows, rows), 0),
        1.0,
        0.0,
    ).astype(BF16)
    before = dot(earlier, (match0 + match1).astype(BF16))
    place0 = first.astype(F32) * cap + jnp.sum(before * match0, axis=1, keepdims=True)
    place1 = second.astype(F32) * cap + jnp.sum(before * match1, axis=1, keepdims=True)
    slot = lax.broadcasted_iota(jnp.int32, (rows, slots), 1).astype(F32)
    pick0 = jnp.where(slot == place0, 1.0, 0.0)
    pick1 = jnp.where(slot == place1, 1.0, 0.0)
    pick[0:rows, :] = pick0.astype(BF16)
    pick[rows : 2 * rows, :] = pick1.astype(BF16)
    either = (pick0 + pick1).astype(BF16)

    side = TILE * TILE
    to = lax.broadcasted_iota(jnp.int32, (side, side), 0)
    come = lax.broadcasted_iota(jnp.int32, (side, side), 1)
    swap[...] = jnp.where(come == lax.rem(to, TILE) * TILE + to // TILE, 1.0, 0.0).astype(BF16)

    wide = 2 * LANES
    for j in range(width // wide):
        columns = pl.ds(j * wide, wide)
        flat[:, columns] = lax.dot_general(
            either, normed[:, columns], (((0,), (0,)), ((), ())), preferred_element_type=F32
        ).astype(BF16)

    def pack(i, carry):
        at = pl.ds(pl.multiple_of(i * TILE, TILE), TILE)
        outgoing[at] = rows_to_tiles(swap[...], lambda columns: flat[at, columns], width)
        return carry

    lax.fori_loop(0, slots // TILE, pack, 0)

    pl.semaphore_wait(barrier, n_ep - 1 + n_tp - 1)

    def send(place, carry):
        target = lax.rem(me + offset_at(place, n_ep), n_ep)
        pltpu.make_async_remote_copy(
            src_ref=outgoing.at[pl.ds(target * cap, cap)],
            dst_ref=arrived.at[pl.ds(place * cap, cap)],
            send_sem=send_sem,
            recv_sem=arrive_sem.at[place // chunk],
            device_id=(target, tp),
            device_id_type=MESH,
        ).start()
        return carry

    lax.fori_loop(0, n_ep - 1, send, 0)
    arrived[pl.ds((n_ep - 1) * cap, cap)] = outgoing[pl.ds(me * cap, cap)]

    shared_parts = ((sh_gate, all_gate), (sh_up, all_up), (sh_down, all_down))
    for n, (block, whole) in enumerate(shared_parts):

        def share(i, carry, n=n, block=block, whole=whole):
            pltpu.make_async_remote_copy(
                src_ref=block,
                dst_ref=whole.at[core, row],
                send_sem=sh_send.at[n],
                recv_sem=sh_recv.at[n],
                device_id=(me, lax.rem(tp + 2 * i, n_tp)),
                device_id_type=MESH,
            ).start()
            return carry

        lax.fori_loop(1, n_row, share, 0)
        whole[core, row] = block[...]

    for copy in weight_copies:
        copy.wait()

    def arrival(n, at):
        return pltpu.make_async_remote_copy(
            src_ref=arrived.at[at], dst_ref=arrived.at[at], send_sem=send_sem,
            recv_sem=arrive_sem.at[n], device_id=(me, tp), device_id_type=MESH,
        )

    def expert_step(n, carry):
        base = pl.multiple_of(n * span, TILE)

        @pl.when(n < n_chunks - 1)
        def _():
            arrival(n, pl.ds(base, span)).wait_recv()

        @pl.when(n == n_chunks - 1)
        def _():
            arrival(n, pl.ds(base, span - cap)).wait_recv()

        for g in range(span // TILE):
            at = pl.ds(g * TILE, TILE)

            def put(columns, values, at=at):
                xs[at, columns] = values

            tiles_to_rows(swap[...], arrived[pl.ds(base + g * TILE, TILE)], put)
        taken = xs[...]
        hidden = silu_mul(dot(taken, wg[...]), dot(taken, wu[...]))
        for j in range(width // 512):
            columns = pl.ds(j * 512, 512)
            rs[:, columns] = dot(hidden, wd[:, columns]).astype(BF16)
        for g in range(span // TILE):
            at = pl.ds(g * TILE, TILE)
            results[pl.ds(base + g * TILE, TILE)] = rows_to_tiles(
                swap[...], lambda columns, at=at: rs[at, columns], width
            )

        def send_back(i, inner):
            place = n * chunk + i
            target = lax.rem(me + n_ep - offset_at(place, n_ep), n_ep)

            @pl.when(place < n_ep - 1)
            def _():
                pltpu.make_async_remote_copy(
                    src_ref=results.at[pl.ds(place * cap, cap)],
                    dst_ref=returned.at[pl.ds(me * cap, cap)],
                    send_sem=back_send,
                    recv_sem=back_recv,
                    device_id=(target, tp),
                    device_id_type=MESH,
                ).start()

            return inner

        lax.fori_loop(0, chunk, send_back, 0)
        return carry

    lax.fori_loop(0, n_chunks, expert_step, 0)
    returned[pl.ds(me * cap, cap)] = results[pl.ds((n_ep - 1) * cap, cap)]

    pair = tp + 1 - 2 * core
    pairs = []
    for n, (block, whole) in enumerate(shared_parts):
        most = whole.at[core, pl.ds(0, n_row - 1)]
        pltpu.make_async_remote_copy(
            src_ref=most, dst_ref=most, send_sem=sh_send.at[n], recv_sem=sh_recv.at[n],
            device_id=(me, tp), device_id_type=MESH,
        ).wait()
        copy = pltpu.make_async_remote_copy(
            src_ref=whole.at[core], dst_ref=whole.at[core], send_sem=pair_send.at[n],
            recv_sem=pair_recv.at[n], device_id=(me, pair), device_id_type=MESH,
        )
        copy.start()
        pairs.append(copy)
    for copy in pairs:
        copy.wait()

    ff = sh_gate.shape[1]
    depth = sh_gate.shape[0]
    gate_sum = jnp.zeros((rows, ff), F32)
    up_sum = jnp.zeros((rows, ff), F32)
    for r in range(n_row):
        part = normed[:, pl.ds(2 * r * depth, 2 * depth)]
        gate_sum += dot(part, jnp.concatenate([all_gate[0, r], all_gate[1, r]], axis=0))
        up_sum += dot(part, jnp.concatenate([all_up[0, r], all_up[1, r]], axis=0))
    shared_hidden = silu_mul(gate_sum, up_sum)
    for r in range(n_row):
        both = jnp.concatenate([all_down[0, r], all_down[1, r]], axis=1)
        shared[:, pl.ds(2 * r * out_width, 2 * out_width)] = dot(shared_hidden, both).astype(BF16)

    rest = pl.ds(0, (n_ep - 1) * cap)
    pltpu.make_async_remote_copy(
        src_ref=results.at[rest], dst_ref=returned.at[rest], send_sem=back_send,
        recv_sem=back_recv, device_id=(me, tp), device_id_type=MESH,
    ).wait()

    def unpack(i, carry):
        at = pl.ds(pl.multiple_of(i * TILE, TILE), TILE)

        def put(columns, values):
            flat[at, columns] = values

        tiles_to_rows(swap[...], returned[at], put)
        return carry

    lax.fori_loop(0, slots // TILE, unpack, 0)
    weight0, weight1 = gates[:, 0:1], gates[:, 1:2]
    squares = jnp.zeros((rows, LANES), F32)
    for j in range(width // wide):
        columns = pl.ds(j * wide, wide)
        picked = dot(pick[...], flat[:, columns])
        routed = (weight0 * picked[0:rows] + weight1 * picked[rows : 2 * rows]).astype(BF16)
        total = routed.astype(F32) + shared[:, columns].astype(F32)
        combined[:, columns] = total
        squares += total[:, 0:LANES] * total[:, 0:LANES] + total[:, LANES:] * total[:, LANES:]
    scale_out = lax.rsqrt(jnp.sum(squares, axis=1, keepdims=True) * (1.0 / width) + 1e-06)
    for j in range(n_tp):
        columns = pl.ds(j * out_width, out_width)
        out_blocks[j] = (combined[:, columns] * scale_out * post_gain[:, columns]).astype(BF16)

    def send_out(i, carry):
        target = lax.rem(tp + i, n_tp)
        pltpu.make_async_remote_copy(
            src_ref=out_blocks.at[target],
            dst_ref=out_landed.at[tp],
            send_sem=out_send,
            recv_sem=out_recv,
            device_id=(me, target),
            device_id_type=MESH,
        ).start()
        return carry

    lax.fori_loop(1, n_tp, send_out, 0)
    out_landed[tp] = out_blocks[tp]

    pltpu.make_async_remote_copy(
        src_ref=outgoing.at[rest], dst_ref=arrived.at[rest], send_sem=send_sem,
        recv_sem=back_recv, device_id=(me, tp), device_id_type=MESH,
    ).wait_send()
    others = pl.ds(0, n_tp - 1)
    pltpu.make_async_remote_copy(
        src_ref=out_blocks.at[others], dst_ref=out_landed.at[others], send_sem=out_send,
        recv_sem=out_recv, device_id=(me, tp), device_id_type=MESH,
    ).wait()
    last = pltpu.make_async_copy(out_landed, out, last_sem)
    last.start()
    last.wait()


def per_device(
    tokens, routes, gates, pre_gain, w_gate, w_up, w_down, sh_gate, sh_up, sh_down, post_gain
):
    rows, width = tokens.shape
    n_ep, n_tp = lax.axis_size("ep"), lax.axis_size("tp")
    ff = w_gate.shape[2]
    cap = max(2, 4 * rows * TOPK // (3 * n_ep))
    chunk = next(c for c in range(2, n_ep) if n_ep % c == 0 and c * cap % TILE == 0)
    slots = n_ep * cap
    n_row = n_tp // 2
    depth, sh_ff = sh_gate.shape
    out_width = width // n_tp
    tiles = pltpu.VMEM((slots, TILE, LANES), BF16)
    vmem = pl.BlockSpec(memory_space=pltpu.VMEM)
    anywhere = pl.BlockSpec(memory_space=pl.ANY)
    dma = pltpu.SemaphoreType.DMA
    result = pl.pallas_call(
        functools.partial(kernel, n_ep, n_tp, cap, chunk),
        out_shape=jax.ShapeDtypeStruct((n_tp, rows, out_width), BF16),
        in_specs=[vmem] * 4 + [anywhere] * 3 + [vmem] * 4,
        out_specs=anywhere,
        scratch_shapes=[
            pltpu.VMEM((rows, width), BF16),
            pltpu.VMEM((2 * rows, slots), BF16),
            pltpu.VMEM((TILE * TILE, TILE * TILE), BF16),
            pltpu.VMEM((slots, width), BF16),
            tiles, tiles, tiles, tiles,
            pltpu.VMEM((width, ff), BF16),
            pltpu.VMEM((width, ff), BF16),
            pltpu.VMEM((ff, width), BF16),
            pltpu.VMEM((chunk * cap, width), BF16),
            pltpu.VMEM((chunk * cap, width), BF16),
            pltpu.VMEM((2, n_row, depth, sh_ff), BF16),
            pltpu.VMEM((2, n_row, depth, sh_ff), BF16),
            pltpu.VMEM((2, n_row, sh_ff, out_width), BF16),
            pltpu.VMEM((rows, width), BF16),
            pltpu.VMEM((rows, width), F32),
            pltpu.VMEM((n_tp, rows, out_width), BF16),
            pltpu.VMEM((n_tp, rows, out_width), BF16),
            dma((3,)), dma, dma((n_ep // chunk,)), dma, dma,
            dma((3,)), dma((3,)), dma((3,)), dma((3,)), dma, dma, dma,
        ],
        compiler_params=pltpu.CompilerParams(
            collective_id=0, has_side_effects=True, vmem_limit_bytes=60 * 1024 * 1024
        ),
    )(
        tokens, routes, gates, pre_gain.reshape(1, width),
        w_gate.reshape(width, ff), w_up.reshape(width, ff), w_down.reshape(ff, width),
        sh_gate, sh_up, sh_down, post_gain.reshape(1, width),
    )
    return result.reshape(n_tp * rows, out_width)


def solution(mesh):
    return jax.shard_map(
        per_device,
        mesh=mesh,
        in_specs=(
            P(("ep", "tp"), None),
            P(("ep", "tp"), None),
            P(("ep", "tp"), None),
            P(),
            P("ep", None, None),
            P("ep", None, None),
            P("ep", None, None),
            P("tp", None),
            P("tp", None),
            P(None, "tp"),
            P(),
        ),
        out_specs=P("ep", "tp"),
        check_vma=False,
    )
```

```python
import functools

import jax
import jax.numpy as jnp
from jax import lax
from jax.experimental import pallas as pl
from jax.experimental.pallas import tpu as pltpu
from jax.sharding import PartitionSpec as P

TOPK = 2
LANES = 128
TILE = 16
N_X = 4
MESH = pl.DeviceIdType.MESH
F32 = jnp.float32
BF16 = jnp.bfloat16


def dot(a, b):
    return jnp.dot(a, b, preferred_element_type=F32)


def silu_mul(gate, up):
    return (gate / (1.0 + jnp.exp(-gate)) * up).astype(BF16)


def offset_at(place, reach, odd):
    groups = 2 * reach
    group, item = place // 4, lax.rem(place, 4)
    first = 1 - (group + groups - 2) // (groups - 1)
    later = group - 1 + first
    ring = first * reach * (1 - 2 * lax.rem(item, 2)) + (1 - first) * (
        (reach - 1 - later // 2) * (1 - 2 * lax.rem(later, 2))
    )
    return ring, first * (2 * (item // 2) + odd) + (1 - first) * item


def swapped(swap, read, blocks):
    stacked = jnp.concatenate([read(b) for b in range(blocks)], axis=0)
    return dot(swap, stacked).astype(BF16)


def order_matrix(outer, inner):
    side = outer * inner
    to = lax.broadcasted_iota(jnp.int32, (side, side), 0)
    come = lax.broadcasted_iota(jnp.int32, (side, side), 1)
    return jnp.where(come == lax.rem(to, inner) * outer + to // inner, 1.0, 0.0).astype(BF16)


def kernel(
    n_ep, n_tp, cap, chunk,
    tokens, routes, gates, pre_gain, w_gate, w_up, w_down, sh_gate, sh_up, sh_down, post_gain,
    out,
    normed, pick, swap, swap_out, swap_in, flat, half_flat, outgoing, arrived, results, returned,
    wg, wu, wd, wg2, wu2, wd2, xs, rs, all_gate, all_up, all_down, shared,
    out_blocks, out_landed, scales, scales_landed,
    w_sem, relay_send, relay_recv, send_sem, arrive_sem, back_send, back_recv,
    ring_send, ring_recv, pair_send, pair_recv,
    out_send, out_recv, scale_send, scale_recv,
):
    me, tp = lax.axis_index("ep"), lax.axis_index("tp")
    core, row = lax.rem(tp, 2), tp // 2
    n_row = n_tp // 2
    n_z = n_ep // N_X
    reach = n_z // 4
    z, x = me // N_X, lax.rem(me, N_X)
    rows, width = tokens.shape
    slots = n_ep * cap
    places = n_ep // 2
    n_chunks = places // chunk
    span = chunk * cap
    own = places - 4
    blocks = width // LANES
    half_blocks = blocks // 2
    half_cap = cap // 2
    other = lax.rem(me + n_ep // 2, n_ep)
    pair = tp + 1 - 2 * core

    def partner(place, odd, sign):
        ring, side = offset_at(place, reach, odd)
        return lax.rem(z + n_z + sign * ring, n_z), lax.rem(x + N_X + sign * side, N_X)

    def remote(source, target, send, receive, device):
        return pltpu.make_async_remote_copy(
            src_ref=source, dst_ref=target, send_sem=send, recv_sem=receive,
            device_id=device, device_id_type=MESH,
        )

    barrier = pltpu.get_barrier_semaphore()

    def greet_ep(i, carry):
        device = (lax.rem(me + i, n_ep), tp)
        pl.semaphore_signal(barrier, inc=1, device_id=device, device_id_type=MESH)
        return carry

    def greet_tp(i, carry):
        device = (me, lax.rem(tp + i, n_tp))
        pl.semaphore_signal(barrier, inc=1, device_id=device, device_id_type=MESH)
        return carry

    lax.fori_loop(1, n_ep, greet_ep, 0)
    lax.fori_loop(1, n_tp, greet_tp, 0)

    weight_copies = [
        pltpu.make_async_copy(source, target, w_sem.at[i])
        for i, (source, target) in enumerate(((w_gate, wg), (w_up, wu), (w_down, wd)))
    ]
    for copy in weight_copies:
        copy.start()
    for copy in weight_copies:
        copy.wait()
    pl.semaphore_wait(barrier, n_ep - 1 + n_tp - 1)

    first_set = (wg, wu, wd)
    second_set = (wg2, wu2, wd2)
    shared_set = (all_gate, all_up, all_down)
    for mine, theirs in zip(first_set, second_set):
        remote(mine.at[tp], theirs.at[tp], relay_send, relay_recv, (other, tp)).start()

    ahead = n_row // 2
    behind = n_row - 1 - ahead
    up_row = 2 * lax.rem(row + 1, n_row) + core
    down_row = 2 * lax.rem(row + n_row - 1, n_row) + core

    def ring_step(k, whole, step, sources=None):
        three = whole[0].at[pl.ds(0, 3)]
        if 1 <= step <= ahead:
            remote(three, three, ring_send.at[k, 0], ring_recv.at[k, 0, step - 1], (me, tp)).wait_recv()
        if 1 <= step <= behind:
            remote(three, three, ring_send.at[k, 1], ring_recv.at[k, 1, step - 1], (me, tp)).wait_recv()
        from_below = 2 * lax.rem(row + n_row - step, n_row) + core
        from_above = 2 * lax.rem(row + step, n_row) + core
        for n, ref in enumerate(whole):
            source = sources[n] if sources is not None else ref.at[from_below]
            if step < ahead:
                remote(
                    source, ref.at[from_below], ring_send.at[k, 0], ring_recv.at[k, 0, step],
                    (me, up_row),
                ).start()
            if step < behind:
                source = sources[n] if sources is not None else ref.at[from_above]
                remote(
                    source, ref.at[from_above], ring_send.at[k, 1], ring_recv.at[k, 1, step],
                    (me, down_row),
                ).start()
        for n, ref in enumerate(whole):
            if step <= ahead:
                source = sources[n] if sources is not None else ref.at[from_below]
                remote(
                    source, ref.at[from_below], pair_send.at[k, n], pair_recv.at[k, n], (me, pair)
                ).start()
            if 1 <= step <= behind:
                remote(
                    ref.at[from_above], ref.at[from_above], pair_send.at[k, n], pair_recv.at[k, n],
                    (me, pair),
                ).start()

    def ring_end(k, whole):
        for n, ref in enumerate(whole):
            part = ref.at[pl.ds(0, n_row)]
            remote(part, part, pair_send.at[k, n], pair_recv.at[k, n], (me, tp)).wait()
        for way, count in ((0, ahead), (1, behind)):
            for n, ref in enumerate(whole):
                if count > 0 and n == 0:
                    part = ref.at[pl.ds(0, 3 * count)]
                    remote(
                        part, part, ring_send.at[k, way], ring_recv.at[k, way, 0], (me, tp)
                    ).wait_send()

    shared_parts = (sh_gate, sh_up, sh_down)
    ring_step(0, shared_set, 0, shared_parts)
    for part, whole in zip(shared_parts, shared_set):
        whole[tp] = part[...]

    def norm_rows(i, carry):
        at = pl.ds(pl.multiple_of(i * TILE, TILE), TILE)
        values = tokens[at, :].astype(F32)
        scale = lax.rsqrt(jnp.mean(values * values, axis=1, keepdims=True) + 1e-06)
        normed[at, :] = (values * scale * pre_gain[...]).astype(BF16)
        return carry

    lax.fori_loop(0, rows // TILE, norm_rows, 0)

    down_at = lax.broadcasted_iota(jnp.int32, (rows, rows), 0)
    across_at = lax.broadcasted_iota(jnp.int32, (rows, rows), 1)
    diagonal = down_at == across_at

    def column(values):
        return jnp.sum(jnp.where(diagonal, values, 0.0), axis=1, keepdims=True)

    expert = lax.broadcasted_iota(jnp.int32, (rows, LANES), 1).astype(F32)
    first = column(routes[0:1, :].astype(F32))
    second = column(routes[1:2, :].astype(F32))
    match0 = jnp.where(first == expert, 1.0, 0.0)
    match1 = jnp.where(second == expert, 1.0, 0.0)
    earlier = jnp.where(across_at < down_at, 1.0, 0.0).astype(BF16)
    before = dot(earlier, (match0 + match1).astype(BF16))
    place0 = first * cap + jnp.sum(before * match0, axis=1, keepdims=True)
    place1 = second * cap + jnp.sum(before * match1, axis=1, keepdims=True)
    slot = lax.broadcasted_iota(jnp.int32, (rows, slots), 1).astype(F32)
    pick0 = jnp.where(slot == place0, 1.0, 0.0)
    pick1 = jnp.where(slot == place1, 1.0, 0.0)
    pick[0:rows, :] = pick0.astype(BF16)
    pick[rows : 2 * rows, :] = pick1.astype(BF16)
    either = (pick0 + pick1).astype(BF16)
    swap[...] = order_matrix(TILE, TILE)
    swap_out[...] = order_matrix(TILE, half_blocks)
    swap_in[...] = order_matrix(half_blocks, TILE)

    wide = 2 * LANES
    for j in range(width // wide):
        columns = pl.ds(j * wide, wide)
        flat[:, columns] = lax.dot_general(
            either, normed[:, columns], (((0,), (0,)), ((), ())), preferred_element_type=F32
        ).astype(BF16)

    def pack(i, carry):
        at = pl.ds(pl.multiple_of(i * TILE, TILE), TILE)
        mixed = swapped(swap[...], lambda b: flat[at, pl.ds(b * LANES, LANES)], blocks)
        outgoing[at] = mixed.reshape(TILE, TILE, LANES)
        return carry

    lax.fori_loop(0, slots // TILE, pack, 0)

    def send_home(place, carry):
        to_z, to_x = partner(place, 0, 1)
        target = to_z * N_X + to_x

        @pl.when(place != own)
        def _():
            remote(
                outgoing.at[pl.ds(target * cap, cap)], arrived.at[pl.ds(place * cap, cap)],
                send_sem, arrive_sem.at[place // chunk], (target, tp),
            ).start()

        return carry

    def send_second(place, carry):
        to_z, to_x = partner(place, 1, 1)
        target = to_z * N_X + to_x
        served = lax.rem(target + n_ep // 2, n_ep)
        there = places + place

        @pl.when(place != own)
        def _():
            remote(
                outgoing.at[pl.ds(served * cap, cap)], arrived.at[pl.ds(there * cap, cap)],
                send_sem, arrive_sem.at[there // chunk], (target, tp),
            ).start()

        return carry

    lax.fori_loop(0, places, send_home, 0)
    lax.fori_loop(0, places, send_second, 0)
    arrived[pl.ds(own * cap, cap)] = outgoing[pl.ds(me * cap, cap)]
    arrived[pl.ds((places + own) * cap, cap)] = outgoing[pl.ds(other * cap, cap)]

    def expert_step(n, weights):
        gate_ref, up_ref, down_ref = weights
        base = n * span
        full = n * chunk // places * places + own < n * chunk or (
            n * chunk // places * places + own >= (n + 1) * chunk
        )
        awaited = arrived.at[pl.ds(base, span if full else span - cap)]
        remote(awaited, awaited, send_sem, arrive_sem.at[n], (me, tp)).wait_recv()
        for g in range(span // TILE):
            at = pl.ds(g * TILE, TILE)
            mixed = swapped(swap[...], lambda b, g=g: arrived[base + g * TILE + b], TILE)
            for b in range(blocks):
                xs[at, pl.ds(b * LANES, LANES)] = mixed[TILE * b : TILE * (b + 1), :]
        taken = xs[...]
        ff = gate_ref.shape[2]
        gate = dot(taken, gate_ref[...].reshape(width, ff))
        hidden = silu_mul(gate, dot(taken, up_ref[...].reshape(width, ff)))
        for j in range(width // 512):
            columns = pl.ds(j * 512, 512)
            rs[:, columns] = dot(hidden, down_ref[:, :, columns].reshape(ff, 512)).astype(BF16)
        for h in range(2):
            for g in range(span // TILE):
                at = pl.ds(g * TILE, TILE)
                mixed = swapped(
                    swap_out[...],
                    lambda b, at=at, h=h: rs[at, pl.ds((2 * b + h) * LANES, LANES)],
                    half_blocks,
                )
                results[h, pl.ds(base // 2 + g * half_blocks, half_blocks)] = mixed.reshape(
                    half_blocks, TILE, LANES
                )

    def send_back(half, start, stop, odd):
        base = odd * places
        served = other if odd else me

        def one(place, carry):
            to_z, to_x = partner(place, odd, -1)

            @pl.when(place != own)
            def _():
                remote(
                    results.at[half, pl.ds((base + place) * half_cap, half_cap)],
                    returned.at[half, pl.ds(served * half_cap, half_cap)],
                    back_send.at[half], back_recv.at[half], (to_z * N_X + to_x, tp),
                ).start()

            return carry

        lax.fori_loop(start, stop, one, 0)

    def keep_own(odd):
        served = other if odd else me
        for h in range(2):
            returned[h, pl.ds(served * half_cap, half_cap)] = results[
                h, pl.ds((odd * places + own) * half_cap, half_cap)
            ]

    early = max(ahead - 1, 1)
    for step in range(1, early):
        ring_step(0, shared_set, step)
    three = wg2.at[pl.ds(0, 3)]
    remote(three, three, relay_send, relay_recv, (me, tp)).wait_recv()
    ring_step(1, second_set, 0)
    for n in range(n_chunks):
        expert_step(n, first_set)
        send_back(0, n * chunk, (n + 1) * chunk, 0)
        if 1 + n < ahead:
            ring_step(1, second_set, 1 + n)
    keep_own(0)
    send_back(1, 0, places, 0)
    for step in range(1 + n_chunks, ahead):
        ring_step(1, second_set, step)
    for step in range(early, ahead):
        ring_step(0, shared_set, step)
    ring_step(1, second_set, ahead)
    ring_end(1, second_set)
    for n in range(n_chunks):
        expert_step(n_chunks + n, second_set)
        send_back(0, n * chunk, (n + 1) * chunk, 1)
    keep_own(1)
    send_back(1, 0, places, 1)

    ring_step(0, shared_set, ahead)
    ring_end(0, shared_set)
    sh_ff = sh_gate.shape[1]
    gate_sum = dot(normed[...], all_gate[...].reshape(width, sh_ff))
    up_sum = dot(normed[...], all_up[...].reshape(width, sh_ff))
    shared_hidden = silu_mul(gate_sum, up_sum)
    out_width = width // n_tp
    for t in range(0, n_tp, 2):
        both = jnp.concatenate([all_down[t], all_down[t + 1]], axis=1)
        shared[:, pl.ds(t * out_width, 2 * out_width)] = dot(shared_hidden, both).astype(BF16)

    weight0, weight1 = column(gates[0:1, :]), column(gates[1:2, :])
    squares = jnp.zeros((rows, LANES), F32)
    for h in range(2):
        rest = pl.ds(0, (n_ep - 2) * half_cap)
        remote(
            results.at[h, rest], returned.at[h, rest], back_send.at[h], back_recv.at[h], (me, tp)
        ).wait_recv()

        def unpack(i, carry, h=h):
            tile = i * half_blocks
            mixed = swapped(swap_in[...], lambda b: returned[h, tile + b], half_blocks)
            at = pl.ds(pl.multiple_of(i * TILE, TILE), TILE)
            for b in range(half_blocks):
                half_flat[at, pl.ds(b * LANES, LANES)] = mixed[TILE * b : TILE * (b + 1), :]
            return carry

        lax.fori_loop(0, slots // TILE, unpack, 0)
        for jj in range(half_blocks // 2):
            picked = dot(pick[...], half_flat[:, pl.ds(jj * wide, wide)])
            routed = (weight0 * picked[0:rows] + weight1 * picked[rows : 2 * rows]).astype(BF16)
            for b in range(2):
                block = 2 * (2 * jj + b) + h
                total = routed[:, b * LANES : (b + 1) * LANES].astype(F32) + shared[
                    :, pl.ds(block * LANES, LANES)
                ].astype(F32)
                squares += total * total
                per = out_width // LANES
                out_blocks[block // per, :, pl.ds(block % per * LANES, LANES)] = total.astype(BF16)
        if out_width == LANES:
            send_out(h, n_row, row, tp, me, remote, out_blocks, out_landed, out_send, out_recv)
    if out_width != LANES:
        for h in range(2):
            send_out(h, n_row, row, tp, me, remote, out_blocks, out_landed, out_send, out_recv)

    scale_out = lax.rsqrt(jnp.sum(squares, axis=1, keepdims=True) * (1.0 / width) + 1e-06)
    scale_line = jnp.sum(jnp.where(diagonal, scale_out, 0.0), axis=0, keepdims=True)
    scales[...] = jnp.broadcast_to(scale_line, scales.shape)

    def send_scale(i, carry):
        target = lax.rem(tp + i, n_tp)
        remote(scales, scales_landed.at[tp], scale_send, scale_recv, (me, target)).start()
        return carry

    lax.fori_loop(1, n_tp, send_scale, 0)
    out_landed[tp] = out_blocks[tp]
    scales_landed[tp] = scales[...]

    remote(three, three, relay_send, relay_recv, (me, tp)).wait_send()
    rest = pl.ds(0, (n_ep - 2) * cap)
    remote(outgoing.at[rest], arrived.at[rest], send_sem, arrive_sem.at[0], (me, tp)).wait_send()
    for h in range(2):
        rest = pl.ds(0, (n_ep - 2) * half_cap)
        remote(
            results.at[h, rest], returned.at[h, rest], back_send.at[h], back_recv.at[h], (me, tp)
        ).wait_send()
    others = pl.ds(0, n_tp - 1)
    some = scales_landed.at[others]
    remote(some, some, scale_send, scale_recv, (me, tp)).wait()
    some = out_landed.at[others]
    remote(some, some, out_send, out_recv, (me, tp)).wait()

    gain = post_gain[:, pl.ds(pl.multiple_of(tp * out_width, LANES), out_width)]

    def finish(t, carry):
        scale = column(scales_landed[t][0:1, :])
        out[t] = (out_landed[t].astype(F32) * scale * gain).astype(BF16)
        return carry

    lax.fori_loop(0, n_tp, finish, 0)


def send_out(h, n_row, row, tp, me, remote, out_blocks, out_landed, out_send, out_recv):
    def one(i, carry):
        target = 2 * lax.rem(row + i, n_row) + h

        @pl.when(target != tp)
        def _():
            remote(
                out_blocks.at[target], out_landed.at[tp], out_send, out_recv, (me, target)
            ).start()

        return carry

    lax.fori_loop(0, n_row, one, 0)


def per_device(
    tokens, routes, gates, pre_gain, w_gate, w_up, w_down, sh_gate, sh_up, sh_down, post_gain
):
    rows, width = tokens.shape
    n_ep, n_tp = lax.axis_size("ep"), lax.axis_size("tp")
    ff = w_gate.shape[2]
    cap = max(2, 4 * rows * TOPK // (3 * n_ep))
    chunk = 8
    slots = n_ep * cap
    n_row = n_tp // 2
    depth, sh_ff = sh_gate.shape
    out_width = width // n_tp
    half_blocks = width // LANES // 2
    vmem = pl.BlockSpec(memory_space=pltpu.VMEM)
    anywhere = pl.BlockSpec(memory_space=pl.ANY)
    dma = pltpu.SemaphoreType.DMA
    tiles = pltpu.VMEM((slots, TILE, LANES), BF16)
    halves = pltpu.VMEM((2, slots // 2, TILE, LANES), BF16)
    in_rows = pltpu.VMEM((n_tp, width // n_tp, ff), BF16)
    out_rows = pltpu.VMEM((n_tp, ff // n_tp, width), BF16)
    result = pl.pallas_call(
        functools.partial(kernel, n_ep, n_tp, cap, chunk),
        out_shape=jax.ShapeDtypeStruct((n_tp, rows, out_width), BF16),
        in_specs=[vmem] * 4 + [anywhere] * 3 + [vmem] * 4,
        out_specs=vmem,
        scratch_shapes=[
            pltpu.VMEM((rows, width), BF16),
            pltpu.VMEM((2 * rows, slots), BF16),
            pltpu.VMEM((TILE * TILE, TILE * TILE), BF16),
            pltpu.VMEM((TILE * half_blocks, TILE * half_blocks), BF16),
            pltpu.VMEM((TILE * half_blocks, TILE * half_blocks), BF16),
            pltpu.VMEM((slots, width), BF16),
            pltpu.VMEM((slots, width // 2), BF16),
            tiles, tiles, halves, halves,
            in_rows, in_rows, out_rows, in_rows, in_rows, out_rows,
            pltpu.VMEM((chunk * cap, width), BF16),
            pltpu.VMEM((chunk * cap, width), BF16),
            pltpu.VMEM((n_tp, depth, sh_ff), BF16),
            pltpu.VMEM((n_tp, depth, sh_ff), BF16),
            pltpu.VMEM((n_tp, sh_ff, out_width), BF16),
            pltpu.VMEM((rows, width), BF16),
            pltpu.VMEM((n_tp, rows, out_width), BF16),
            pltpu.VMEM((n_tp, rows, out_width), BF16),
            pltpu.VMEM((8, rows), F32),
            pltpu.VMEM((n_tp, 8, rows), F32),
            dma((3,)), dma, dma, dma, dma((n_ep // chunk,)), dma((2,)), dma((2,)),
            dma((2, 2)), dma((2, 2, n_row // 2)), dma((2, 3)), dma((2, 3)),
            dma, dma, dma, dma,
        ],
        compiler_params=pltpu.CompilerParams(
            collective_id=0, has_side_effects=True, vmem_limit_bytes=60 * 1024 * 1024
        ),
    )(
        tokens, routes.T, gates.T, pre_gain.reshape(1, width),
        w_gate.reshape(n_tp, width // n_tp, ff), w_up.reshape(n_tp, width // n_tp, ff),
        w_down.reshape(n_tp, ff // n_tp, width),
        sh_gate, sh_up, sh_down, post_gain.reshape(1, width),
    )
    return result.reshape(n_tp * rows, out_width)


def solution(mesh):
    return jax.shard_map(
        per_device,
        mesh=mesh,
        in_specs=(
            P(("ep", "tp"), None),
            P(("ep", "tp"), None),
            P(("ep", "tp"), None),
            P(),
            P("ep", None, None),
            P("ep", None, None),
            P("ep", None, None),
            P("tp", None),
            P("tp", None),
            P(None, "tp"),
            P(),
        ),
        out_specs=P("ep", "tp"),
        check_vma=False,
    )
```

```python
import functools

import jax
import jax.numpy as jnp
from jax import lax
from jax.experimental import pallas as pl
from jax.experimental.pallas import tpu as pltpu
from jax.sharding import PartitionSpec as P

TOPK = 2
LANES = 128
TILE = 16
N_X = 4
MESH = pl.DeviceIdType.MESH
F32 = jnp.float32
BF16 = jnp.bfloat16


def dot(a, b):
    return jnp.dot(a, b, preferred_element_type=F32)


def silu_mul(gate, up):
    return (gate / (1.0 + jnp.exp(-gate)) * up).astype(BF16)


def offset_at(place, reach, odd):
    groups = 2 * reach
    group, item = place // 4, lax.rem(place, 4)
    first = 1 - (group + groups - 2) // (groups - 1)
    later = group - 1 + first
    ring = first * reach * (1 - 2 * lax.rem(item, 2)) + (1 - first) * (
        (reach - 1 - later // 2) * (1 - 2 * lax.rem(later, 2))
    )
    return ring, first * (2 * (item // 2) + odd) + (1 - first) * item


def swapped(swap, read, blocks):
    stacked = jnp.concatenate([read(b) for b in range(blocks)], axis=0)
    return dot(swap, stacked).astype(BF16)


def order_matrix(outer, inner):
    side = outer * inner
    to = lax.broadcasted_iota(jnp.int32, (side, side), 0)
    come = lax.broadcasted_iota(jnp.int32, (side, side), 1)
    return jnp.where(come == lax.rem(to, inner) * outer + to // inner, 1.0, 0.0).astype(BF16)


def kernel(
    n_ep, n_tp, cap, chunk,
    tokens_in, routes_in, gates_in, pre_gain_in, w_gate, w_up, w_down, sh_gate, sh_up, sh_down,
    out_landed, scales_landed,
    tokens, routes, gates, pre_gain, slice_gate, slice_up, slice_down,
    normed, pick, swap, swap_out, swap_in, flat, half_flat, outgoing, arrived, results, returned,
    wg, wu, wd, wg2, wu2, wd2, xs, rs, all_gate, all_up, all_down, shared,
    out_blocks, scales,
    in_sem, w_sem, relay_send, relay_recv, send_sem, arrive_sem, back_send, back_recv,
    ring_send, ring_recv, pair_send, pair_recv,
    out_send, out_recv, scale_send, scale_recv,
):
    me, tp = lax.axis_index("ep"), lax.axis_index("tp")
    core, row = lax.rem(tp, 2), tp // 2
    n_row = n_tp // 2
    n_z = n_ep // N_X
    reach = n_z // 4
    z, x = me // N_X, lax.rem(me, N_X)
    rows, width = tokens.shape
    slots = n_ep * cap
    unroll = next(u for u in (5, 4, 3, 2, 1) if slots // TILE % u == 0)
    places = n_ep // 2
    n_chunks = places // chunk
    span = chunk * cap
    own = places - 4
    blocks = width // LANES
    half_blocks = blocks // 2
    half_cap = cap // 2
    other = lax.rem(me + n_ep // 2, n_ep)
    pair = tp + 1 - 2 * core

    def partner(place, odd, sign):
        ring, side = offset_at(place, reach, odd)
        return lax.rem(z + n_z + sign * ring, n_z), lax.rem(x + N_X + sign * side, N_X)

    def remote(source, target, send, receive, device):
        return pltpu.make_async_remote_copy(
            src_ref=source, dst_ref=target, send_sem=send, recv_sem=receive,
            device_id=device, device_id_type=MESH,
        )

    barrier = pltpu.get_barrier_semaphore()

    def greet_ep(i, carry):
        device = (lax.rem(me + i, n_ep), tp)
        pl.semaphore_signal(barrier, inc=1, device_id=device, device_id_type=MESH)
        return carry

    def greet_tp(i, carry):
        device = (me, lax.rem(tp + i, n_tp))
        pl.semaphore_signal(barrier, inc=1, device_id=device, device_id_type=MESH)
        return carry

    first_set = (wg, wu, wd)
    second_set = (wg2, wu2, wd2)
    shared_set = (all_gate, all_up, all_down)
    slices = (slice_gate, slice_up, slice_down)
    loads = [
        pltpu.make_async_copy(source, target, in_sem.at[i])
        for i, (source, target) in enumerate(
            (
                (tokens_in, tokens), (pre_gain_in, pre_gain), (routes_in, routes),
                (gates_in, gates),
                (w_gate.at[tp], slice_gate), (w_up.at[tp], slice_up), (w_down.at[tp], slice_down),
                (sh_gate, all_gate.at[tp]), (sh_up, all_up.at[tp]), (sh_down, all_down.at[tp]),
            )
        )
    ]
    for copy in loads:
        copy.start()
    lax.fori_loop(1, n_ep, greet_ep, 0)
    lax.fori_loop(1, n_tp, greet_tp, 0)
    weight_copies = [
        pltpu.make_async_copy(source, target, w_sem.at[i])
        for i, (source, target) in enumerate(zip((w_gate, w_up, w_down), first_set))
    ]
    for copy in weight_copies:
        copy.start()
    for copy in loads[:4]:
        copy.wait()

    ahead = n_row // 2
    behind = n_row - 1 - ahead
    up_row = 2 * lax.rem(row + 1, n_row) + core
    down_row = 2 * lax.rem(row + n_row - 1, n_row) + core

    def ring_step(k, whole, step):
        three = whole[0].at[pl.ds(0, 3)]
        if 1 <= step <= ahead:
            remote(three, three, ring_send.at[k, 0], ring_recv.at[k, 0, step - 1], (me, tp)).wait_recv()
        if 1 <= step <= behind:
            remote(three, three, ring_send.at[k, 1], ring_recv.at[k, 1, step - 1], (me, tp)).wait_recv()
        from_below = 2 * lax.rem(row + n_row - step, n_row) + core
        from_above = 2 * lax.rem(row + step, n_row) + core
        for n, ref in enumerate(whole):
            source = ref.at[from_below]
            if step < ahead:
                remote(
                    source, ref.at[from_below], ring_send.at[k, 0], ring_recv.at[k, 0, step],
                    (me, up_row),
                ).start()
            if step < behind:
                source = ref.at[from_above]
                remote(
                    source, ref.at[from_above], ring_send.at[k, 1], ring_recv.at[k, 1, step],
                    (me, down_row),
                ).start()
        for n, ref in enumerate(whole):
            if step <= ahead:
                source = ref.at[from_below]
                remote(
                    source, ref.at[from_below], pair_send.at[k, n], pair_recv.at[k, n], (me, pair)
                ).start()
            if 1 <= step <= behind:
                remote(
                    ref.at[from_above], ref.at[from_above], pair_send.at[k, n], pair_recv.at[k, n],
                    (me, pair),
                ).start()

    def ring_end(k, whole):
        for n, ref in enumerate(whole):
            part = ref.at[pl.ds(0, n_row)]
            remote(part, part, pair_send.at[k, n], pair_recv.at[k, n], (me, tp)).wait()
        for way, count in ((0, ahead), (1, behind)):
            for n, ref in enumerate(whole):
                if count > 0 and n == 0:
                    part = ref.at[pl.ds(0, 3 * count)]
                    remote(
                        part, part, ring_send.at[k, way], ring_recv.at[k, way, 0], (me, tp)
                    ).wait_send()

    def norm_rows(i, carry):
        at = pl.ds(pl.multiple_of(i * 3 * TILE, TILE), 3 * TILE)
        values = tokens[at, :].astype(F32)
        scale = lax.rsqrt(jnp.mean(values * values, axis=1, keepdims=True) + 1e-06)
        normed[at, :] = (values * scale * pre_gain[...]).astype(BF16)
        return carry

    lax.fori_loop(0, rows // (3 * TILE), norm_rows, 0)

    down_at = lax.broadcasted_iota(jnp.int32, (rows, rows), 0)
    across_at = lax.broadcasted_iota(jnp.int32, (rows, rows), 1)
    diagonal = down_at == across_at

    def column(values):
        return jnp.sum(jnp.where(diagonal, values, 0.0), axis=1, keepdims=True)

    expert = lax.broadcasted_iota(jnp.int32, (rows, LANES), 1).astype(F32)
    first = column(routes[0:1, :].astype(F32))
    second = column(routes[1:2, :].astype(F32))
    match0 = jnp.where(first == expert, 1.0, 0.0)
    match1 = jnp.where(second == expert, 1.0, 0.0)
    earlier = jnp.where(across_at < down_at, 1.0, 0.0).astype(BF16)
    before = dot(earlier, (match0 + match1).astype(BF16))
    place0 = first * cap + jnp.sum(before * match0, axis=1, keepdims=True)
    place1 = second * cap + jnp.sum(before * match1, axis=1, keepdims=True)
    slot = lax.broadcasted_iota(jnp.int32, (rows, slots), 1).astype(F32)
    pick0 = jnp.where(slot == place0, 1.0, 0.0)
    pick1 = jnp.where(slot == place1, 1.0, 0.0)
    pick[0:rows, :] = pick0.astype(BF16)
    pick[rows : 2 * rows, :] = pick1.astype(BF16)
    either = (pick0 + pick1).astype(BF16)
    for copy in loads[4:]:
        copy.wait()
    pl.semaphore_wait(barrier, n_ep - 1 + n_tp - 1)

    for mine, theirs in zip(slices, second_set):
        remote(mine, theirs.at[tp], relay_send, relay_recv, (other, tp)).start()
    ring_step(0, shared_set, 0)

    swap[...] = order_matrix(TILE, TILE)
    swap_out[...] = order_matrix(TILE, half_blocks)
    swap_in[...] = order_matrix(half_blocks, TILE)

    wide = 2 * LANES
    for j in range(width // wide):
        columns = pl.ds(j * wide, wide)
        flat[:, columns] = lax.dot_general(
            either, normed[:, columns], (((0,), (0,)), ((), ())), preferred_element_type=F32
        ).astype(BF16)

    def pack(i, carry):
        for u in range(unroll):
            at = pl.ds(pl.multiple_of((i * unroll + u) * TILE, TILE), TILE)
            mixed = swapped(
                swap[...], lambda b, at=at: flat[at, pl.ds(b * LANES, LANES)], blocks
            )
            outgoing[at] = mixed.reshape(TILE, TILE, LANES)
        return carry

    lax.fori_loop(0, slots // TILE // unroll, pack, 0)

    def send_home(place, carry):
        to_z, to_x = partner(place, 0, 1)
        target = to_z * N_X + to_x

        @pl.when(place != own)
        def _():
            remote(
                outgoing.at[pl.ds(target * cap, cap)], arrived.at[pl.ds(place * cap, cap)],
                send_sem, arrive_sem.at[place // chunk], (target, tp),
            ).start()

        return carry

    def send_second(place, carry):
        to_z, to_x = partner(place, 1, 1)
        target = to_z * N_X + to_x
        served = lax.rem(target + n_ep // 2, n_ep)
        there = places + place

        @pl.when(place != own)
        def _():
            remote(
                outgoing.at[pl.ds(served * cap, cap)], arrived.at[pl.ds(there * cap, cap)],
                send_sem, arrive_sem.at[there // chunk], (target, tp),
            ).start()

        return carry

    lax.fori_loop(0, places, send_home, 0)
    lax.fori_loop(0, places, send_second, 0)
    arrived[pl.ds(own * cap, cap)] = outgoing[pl.ds(me * cap, cap)]
    arrived[pl.ds((places + own) * cap, cap)] = outgoing[pl.ds(other * cap, cap)]

    def expert_step(n, weights):
        gate_ref, up_ref, down_ref = weights
        base = n * span
        full = n * chunk // places * places + own < n * chunk or (
            n * chunk // places * places + own >= (n + 1) * chunk
        )
        awaited = arrived.at[pl.ds(base, span if full else span - cap)]
        remote(awaited, awaited, send_sem, arrive_sem.at[n], (me, tp)).wait_recv()
        for g in range(span // TILE):
            at = pl.ds(g * TILE, TILE)
            mixed = swapped(swap[...], lambda b, g=g: arrived[base + g * TILE + b], TILE)
            for b in range(blocks):
                xs[at, pl.ds(b * LANES, LANES)] = mixed[TILE * b : TILE * (b + 1), :]
        taken = xs[...]
        ff = gate_ref.shape[2]
        gate = dot(taken, gate_ref[...].reshape(width, ff))
        hidden = silu_mul(gate, dot(taken, up_ref[...].reshape(width, ff)))
        for j in range(width // 512):
            columns = pl.ds(j * 512, 512)
            rs[:, columns] = dot(hidden, down_ref[:, :, columns].reshape(ff, 512)).astype(BF16)
        for h in range(2):
            for g in range(span // TILE):
                at = pl.ds(g * TILE, TILE)
                mixed = swapped(
                    swap_out[...],
                    lambda b, at=at, h=h: rs[at, pl.ds((2 * b + h) * LANES, LANES)],
                    half_blocks,
                )
                results[h, pl.ds(base // 2 + g * half_blocks, half_blocks)] = mixed.reshape(
                    half_blocks, TILE, LANES
                )

    def send_back(half, start, stop, odd):
        base = odd * places
        served = other if odd else me

        def one(place, carry):
            to_z, to_x = partner(place, odd, -1)

            @pl.when(place != own)
            def _():
                remote(
                    results.at[half, pl.ds((base + place) * half_cap, half_cap)],
                    returned.at[half, pl.ds(served * half_cap, half_cap)],
                    back_send.at[half], back_recv.at[half], (to_z * N_X + to_x, tp),
                ).start()

            return carry

        lax.fori_loop(start, stop, one, 0)

    def keep_own(odd):
        served = other if odd else me
        for h in range(2):
            returned[h, pl.ds(served * half_cap, half_cap)] = results[
                h, pl.ds((odd * places + own) * half_cap, half_cap)
            ]

    early = max(ahead - 1, 1)
    for step in range(1, early):
        ring_step(0, shared_set, step)
    three = wg2.at[pl.ds(0, 3)]
    remote(three, three, relay_send, relay_recv, (me, tp)).wait_recv()
    ring_step(1, second_set, 0)
    for copy in weight_copies:
        copy.wait()
    for n in range(n_chunks):
        if 1 + n < ahead:
            ring_step(1, second_set, 1 + n)
        expert_step(n, first_set)
        send_back(0, n * chunk, (n + 1) * chunk, 0)
    for step in range(1 + n_chunks, ahead):
        ring_step(1, second_set, step)
    for step in range(early, ahead):
        ring_step(0, shared_set, step)
    keep_own(0)
    send_back(1, 0, places, 0)
    ring_step(1, second_set, ahead)
    ring_end(1, second_set)
    for n in range(n_chunks):
        expert_step(n_chunks + n, second_set)
        send_back(0, n * chunk, (n + 1) * chunk, 1)
    keep_own(1)
    send_back(1, 0, places, 1)

    ring_step(0, shared_set, ahead)
    ring_end(0, shared_set)
    sh_ff = all_gate.shape[2]
    gate_sum = dot(normed[...], all_gate[...].reshape(width, sh_ff))
    up_sum = dot(normed[...], all_up[...].reshape(width, sh_ff))
    shared_hidden = silu_mul(gate_sum, up_sum)
    out_width = width // n_tp
    for t in range(0, n_tp, 2):
        both = jnp.concatenate([all_down[t], all_down[t + 1]], axis=1)
        shared[:, pl.ds(t * out_width, 2 * out_width)] = dot(shared_hidden, both).astype(BF16)

    weight0, weight1 = column(gates[0:1, :]), column(gates[1:2, :])
    squares = jnp.zeros((rows, LANES), F32)
    for h in range(2):
        rest = pl.ds(0, (n_ep - 2) * half_cap)
        remote(
            results.at[h, rest], returned.at[h, rest], back_send.at[h], back_recv.at[h], (me, tp)
        ).wait_recv()

        def unpack(i, carry, h=h):
            for u in range(unroll):
                group = i * unroll + u
                tile = group * half_blocks
                mixed = swapped(
                    swap_in[...], lambda b, tile=tile: returned[h, tile + b], half_blocks
                )
                at = pl.ds(pl.multiple_of(group * TILE, TILE), TILE)
                for b in range(half_blocks):
                    half_flat[at, pl.ds(b * LANES, LANES)] = mixed[TILE * b : TILE * (b + 1), :]
            return carry

        lax.fori_loop(0, slots // TILE // unroll, unpack, 0)
        for jj in range(half_blocks // 2):
            picked = dot(pick[...], half_flat[:, pl.ds(jj * wide, wide)])
            routed = (weight0 * picked[0:rows] + weight1 * picked[rows : 2 * rows]).astype(BF16)
            for b in range(2):
                block = 2 * (2 * jj + b) + h
                total = routed[:, b * LANES : (b + 1) * LANES].astype(F32) + shared[
                    :, pl.ds(block * LANES, LANES)
                ].astype(F32)
                squares += total * total
                per = out_width // LANES
                out_blocks[block // per, :, pl.ds(block % per * LANES, LANES)] = total.astype(BF16)
        if out_width == LANES:
            send_out(h, n_row, row, tp, me, remote, out_blocks, out_landed, out_send, out_recv)
    if out_width != LANES:
        for h in range(2):
            send_out(h, n_row, row, tp, me, remote, out_blocks, out_landed, out_send, out_recv)

    scale_out = lax.rsqrt(jnp.sum(squares, axis=1, keepdims=True) * (1.0 / width) + 1e-06)
    scale_line = jnp.sum(jnp.where(diagonal, scale_out, 0.0), axis=0, keepdims=True)
    scales[...] = jnp.broadcast_to(scale_line, scales.shape)

    def send_scale(i, carry):
        target = lax.rem(tp + i, n_tp)
        remote(scales, scales_landed.at[tp], scale_send, scale_recv, (me, target)).start()
        return carry

    lax.fori_loop(1, n_tp, send_scale, 0)
    out_landed[tp] = out_blocks[tp]
    scales_landed[tp] = scales[...]

    remote(three, three, relay_send, relay_recv, (me, tp)).wait_send()
    rest = pl.ds(0, (n_ep - 2) * cap)
    remote(outgoing.at[rest], arrived.at[rest], send_sem, arrive_sem.at[0], (me, tp)).wait_send()
    for h in range(2):
        rest = pl.ds(0, (n_ep - 2) * half_cap)
        remote(
            results.at[h, rest], returned.at[h, rest], back_send.at[h], back_recv.at[h], (me, tp)
        ).wait_send()
    others = pl.ds(0, n_tp - 1)
    some = scales_landed.at[others]
    remote(some, some, scale_send, scale_recv, (me, tp)).wait()
    some = out_landed.at[others]
    remote(some, some, out_send, out_recv, (me, tp)).wait()


def finish(landed, scales, post_gain, out):
    sources, rows, out_width = landed.shape
    at = pl.multiple_of(lax.axis_index("tp") * out_width, LANES)
    gain = post_gain[:, pl.ds(at, out_width)]
    down_at = lax.broadcasted_iota(jnp.int32, (rows, rows), 0)
    diagonal = down_at == lax.broadcasted_iota(jnp.int32, (rows, rows), 1)
    for t in range(sources):
        scale = jnp.sum(jnp.where(diagonal, scales[t, 0:1, :], 0.0), axis=1, keepdims=True)
        out[t] = (landed[t].astype(F32) * scale * gain).astype(BF16)


def send_out(h, n_row, row, tp, me, remote, out_blocks, out_landed, out_send, out_recv):
    def one(i, carry):
        target = 2 * lax.rem(row + i, n_row) + h

        @pl.when(target != tp)
        def _():
            remote(
                out_blocks.at[target], out_landed.at[tp], out_send, out_recv, (me, target)
            ).start()

        return carry

    lax.fori_loop(0, n_row, one, 0)


def per_device(
    tokens, routes, gates, pre_gain, w_gate, w_up, w_down, sh_gate, sh_up, sh_down, post_gain
):
    rows, width = tokens.shape
    n_ep, n_tp = lax.axis_size("ep"), lax.axis_size("tp")
    ff = w_gate.shape[2]
    cap = max(2, 4 * rows * TOPK // (3 * n_ep))
    chunk = 8
    slots = n_ep * cap
    n_row = n_tp // 2
    depth, sh_ff = sh_gate.shape
    out_width = width // n_tp
    half_blocks = width // LANES // 2
    vmem = pl.BlockSpec(memory_space=pltpu.VMEM)
    anywhere = pl.BlockSpec(memory_space=pl.ANY)
    dma = pltpu.SemaphoreType.DMA
    tiles = pltpu.VMEM((slots, TILE, LANES), BF16)
    halves = pltpu.VMEM((2, slots // 2, TILE, LANES), BF16)
    in_rows = pltpu.VMEM((n_tp, width // n_tp, ff), BF16)
    out_rows = pltpu.VMEM((n_tp, ff // n_tp, width), BF16)
    landed, scales = pl.pallas_call(
        functools.partial(kernel, n_ep, n_tp, cap, chunk),
        out_shape=(
            jax.ShapeDtypeStruct((n_tp, rows, out_width), BF16),
            jax.ShapeDtypeStruct((n_tp, 8, rows), F32),
        ),
        in_specs=[anywhere] * 10,
        out_specs=(vmem, vmem),
        scratch_shapes=[
            pltpu.VMEM((rows, width), BF16),
            pltpu.VMEM((2, rows), jnp.int32),
            pltpu.VMEM((2, rows), F32),
            pltpu.VMEM((1, width), F32),
            pltpu.VMEM((width // n_tp, ff), BF16),
            pltpu.VMEM((width // n_tp, ff), BF16),
            pltpu.VMEM((ff // n_tp, width), BF16),
            pltpu.VMEM((rows, width), BF16),
            pltpu.VMEM((2 * rows, slots), BF16),
            pltpu.VMEM((TILE * TILE, TILE * TILE), BF16),
            pltpu.VMEM((TILE * half_blocks, TILE * half_blocks), BF16),
            pltpu.VMEM((TILE * half_blocks, TILE * half_blocks), BF16),
            pltpu.VMEM((slots, width), BF16),
            pltpu.VMEM((slots, width // 2), BF16),
            tiles, tiles, halves, halves,
            in_rows, in_rows, out_rows, in_rows, in_rows, out_rows,
            pltpu.VMEM((chunk * cap, width), BF16),
            pltpu.VMEM((chunk * cap, width), BF16),
            pltpu.VMEM((n_tp, depth, sh_ff), BF16),
            pltpu.VMEM((n_tp, depth, sh_ff), BF16),
            pltpu.VMEM((n_tp, sh_ff, out_width), BF16),
            pltpu.VMEM((rows, width), BF16),
            pltpu.VMEM((n_tp, rows, out_width), BF16),
            pltpu.VMEM((8, rows), F32),
            dma((10,)), dma((3,)), dma, dma, dma, dma((n_ep // chunk,)), dma((2,)), dma((2,)),
            dma((2, 2)), dma((2, 2, n_row // 2)), dma((2, 3)), dma((2, 3)),
            dma, dma, dma, dma,
        ],
        compiler_params=pltpu.CompilerParams(
            collective_id=0, has_side_effects=True, vmem_limit_bytes=60 * 1024 * 1024
        ),
    )(
        tokens, routes.T, gates.T, pre_gain.reshape(1, width),
        w_gate.reshape(n_tp, width // n_tp, ff), w_up.reshape(n_tp, width // n_tp, ff),
        w_down.reshape(n_tp, ff // n_tp, width),
        sh_gate, sh_up, sh_down,
    )
    some = n_tp // 4
    result = pl.pallas_call(
        finish,
        grid=(4,),
        out_shape=jax.ShapeDtypeStruct((n_tp, rows, out_width), BF16),
        in_specs=[
            pl.BlockSpec((some, rows, out_width), lambda i: (i, 0, 0)),
            pl.BlockSpec((some, 8, rows), lambda i: (i, 0, 0)),
            pl.BlockSpec((1, width), lambda i: (0, 0)),
        ],
        out_specs=pl.BlockSpec((some, rows, out_width), lambda i: (i, 0, 0)),
    )(landed, scales, post_gain.reshape(1, width))
    return result.reshape(n_tp * rows, out_width)


def solution(mesh):
    return jax.shard_map(
        per_device,
        mesh=mesh,
        in_specs=(
            P(("ep", "tp"), None),
            P(("ep", "tp"), None),
            P(("ep", "tp"), None),
            P(),
            P("ep", None, None),
            P("ep", None, None),
            P("ep", None, None),
            P("tp", None),
            P("tp", None),
            P(None, "tp"),
            P(),
        ),
        out_specs=P("ep", "tp"),
        check_vma=False,
    )
```

```python
import functools

import jax
import jax.numpy as jnp
from jax import lax
from jax.experimental import pallas as pl
from jax.experimental.pallas import tpu as pltpu
from jax.sharding import PartitionSpec as P

TOPK = 2
LANES = 128
TILE = 16
N_X = 4
MESH = pl.DeviceIdType.MESH
F32 = jnp.float32
BF16 = jnp.bfloat16


def dot(a, b):
    return jnp.dot(a, b, preferred_element_type=F32)


def silu_mul(gate, up):
    return (gate / (1.0 + jnp.exp(-gate)) * up).astype(BF16)


def offset_at(place, reach, odd):
    groups = 2 * reach
    group, item = place // 4, lax.rem(place, 4)
    first = 1 - (group + groups - 2) // (groups - 1)
    later = group - 1 + first
    ring = first * reach * (1 - 2 * lax.rem(item, 2)) + (1 - first) * (
        (reach - 1 - later // 2) * (1 - 2 * lax.rem(later, 2))
    )
    return ring, first * (2 * (item // 2) + odd) + (1 - first) * item


def swapped(swap, read, blocks):
    stacked = jnp.concatenate([read(b) for b in range(blocks)], axis=0)
    return dot(swap, stacked).astype(BF16)


def order_matrix(outer, inner):
    side = outer * inner
    to = lax.broadcasted_iota(jnp.int32, (side, side), 0)
    come = lax.broadcasted_iota(jnp.int32, (side, side), 1)
    return jnp.where(come == lax.rem(to, inner) * outer + to // inner, 1.0, 0.0).astype(BF16)


def kernel(
    n_ep, n_tp, cap, chunk,
    tokens_in, routes_in, gates_in, pre_gain_in, w_gate, w_up, w_down, sh_gate, sh_up, sh_down,
    out_landed, scales_landed,
    tokens, routes, gates, pre_gain, slice_gate, slice_up, slice_down,
    normed, pick, swap, swap_out, swap_in, flat, half_flat, outgoing, arrived, results, returned,
    wg, wu, wd, wg2, wu2, wd2, xs, rs, all_gate, all_up, all_down, shared,
    out_blocks, scales,
    in_sem, w_sem, relay_send, relay_recv, send_sem, arrive_sem, back_send, back_recv,
    ring_send, ring_recv, pair_send, pair_recv,
    out_send, out_recv, scale_send, scale_recv,
):
    me, tp = lax.axis_index("ep"), lax.axis_index("tp")
    core, row = lax.rem(tp, 2), tp // 2
    n_row = n_tp // 2
    n_z = n_ep // N_X
    reach = n_z // 4
    z, x = me // N_X, lax.rem(me, N_X)
    rows, width = tokens.shape
    slots = n_ep * cap
    unroll = next(u for u in (5, 4, 3, 2, 1) if slots // TILE % u == 0)
    places = n_ep // 2
    n_chunks = places // chunk
    span = chunk * cap
    own = places - 4
    blocks = width // LANES
    half_blocks = blocks // 2
    half_cap = cap // 2
    other = lax.rem(me + n_ep // 2, n_ep)
    pair = tp + 1 - 2 * core

    def partner(place, odd, sign):
        ring, side = offset_at(place, reach, odd)
        return lax.rem(z + n_z + sign * ring, n_z), lax.rem(x + N_X + sign * side, N_X)

    def remote(source, target, send, receive, device):
        return pltpu.make_async_remote_copy(
            src_ref=source, dst_ref=target, send_sem=send, recv_sem=receive,
            device_id=device, device_id_type=MESH,
        )

    barrier = pltpu.get_barrier_semaphore()

    near = (2 * reach + 1) * N_X
    itself = reach * N_X

    def greet_near(i, carry):
        at_z = lax.rem(z + n_z + i // N_X - reach, n_z)
        device = (at_z * N_X + lax.rem(x + lax.rem(i, N_X), N_X), tp)
        pl.semaphore_signal(barrier, inc=1, device_id=device, device_id_type=MESH)
        return carry

    def greet_tp(i, carry):
        device = (me, lax.rem(tp + i, n_tp))
        pl.semaphore_signal(barrier, inc=1, device_id=device, device_id_type=MESH)
        return carry

    first_set = (wg, wu, wd)
    second_set = (wg2, wu2, wd2)
    shared_set = (all_gate, all_up, all_down)
    slices = (slice_gate, slice_up, slice_down)
    loads = [
        pltpu.make_async_copy(source, target, in_sem.at[i])
        for i, (source, target) in enumerate(
            (
                (tokens_in, tokens), (pre_gain_in, pre_gain), (routes_in, routes),
                (gates_in, gates),
                (w_gate.at[tp], slice_gate), (w_up.at[tp], slice_up), (w_down.at[tp], slice_down),
                (sh_gate, all_gate.at[tp]), (sh_up, all_up.at[tp]), (sh_down, all_down.at[tp]),
            )
        )
    ]
    for copy in loads:
        copy.start()
    pl.semaphore_signal(barrier, inc=1, device_id=(other, tp), device_id_type=MESH)
    lax.fori_loop(0, itself, greet_near, 0)
    lax.fori_loop(itself + 1, near, greet_near, 0)
    lax.fori_loop(1, n_tp, greet_tp, 0)
    weight_copies = [
        pltpu.make_async_copy(source, target, w_sem.at[i])
        for i, (source, target) in enumerate(zip((w_gate, w_up, w_down), first_set))
    ]
    for copy in weight_copies:
        copy.start()
    for copy in loads[:4]:
        copy.wait()

    ahead = n_row // 2
    behind = n_row - 1 - ahead
    up_row = 2 * lax.rem(row + 1, n_row) + core
    down_row = 2 * lax.rem(row + n_row - 1, n_row) + core

    def ring_step(k, whole, n, step):
        ref = whole[n]
        ups, downs = (ahead, behind) if n < 2 else (behind, ahead)
        below = ref.at[2 * lax.rem(row + n_row - step, n_row) + core]
        above = ref.at[2 * lax.rem(row + step, n_row) + core]
        ways = ((0, below, ups, up_row), (1, above, downs, down_row))
        for way, block, hops, _ in ways:
            if 1 <= step <= hops:
                receive = ring_recv.at[3 * k + n, way, step - 1]
                remote(block, block, ring_send.at[k, way], receive, (me, tp)).wait_recv()
        for way, block, hops, target in ways:
            if step < hops:
                receive = ring_recv.at[3 * k + n, way, step]
                remote(block, block, ring_send.at[k, way], receive, (me, target)).start()
        for way, block, hops, _ in ways:
            if way <= step <= hops:
                remote(block, block, pair_send.at[k, n], pair_recv.at[k, n], (me, pair)).start()

    def ring_end(k, whole):
        for n, ref in enumerate(whole):
            part = ref.at[pl.ds(0, n_row)]
            remote(part, part, pair_send.at[k, n], pair_recv.at[k, n], (me, tp)).wait()
        for way, count in ((0, 2 * ahead + behind), (1, 2 * behind + ahead)):
            part = whole[0].at[pl.ds(0, count)]
            receive = ring_recv.at[3 * k, way, 0]
            remote(part, part, ring_send.at[k, way], receive, (me, tp)).wait_send()

    def norm_rows(i, carry):
        at = pl.ds(pl.multiple_of(i * 3 * TILE, TILE), 3 * TILE)
        values = tokens[at, :].astype(F32)
        scale = lax.rsqrt(jnp.mean(values * values, axis=1, keepdims=True) + 1e-06)
        normed[at, :] = (values * scale * pre_gain[...]).astype(BF16)
        return carry

    lax.fori_loop(0, rows // (3 * TILE), norm_rows, 0)

    down_at = lax.broadcasted_iota(jnp.int32, (rows, rows), 0)
    across_at = lax.broadcasted_iota(jnp.int32, (rows, rows), 1)
    diagonal = down_at == across_at

    def column(values):
        return jnp.sum(jnp.where(diagonal, values, 0.0), axis=1, keepdims=True)

    expert = lax.broadcasted_iota(jnp.int32, (rows, LANES), 1).astype(F32)
    first = column(routes[0:1, :].astype(F32))
    second = column(routes[1:2, :].astype(F32))
    match0 = jnp.where(first == expert, 1.0, 0.0)
    match1 = jnp.where(second == expert, 1.0, 0.0)
    earlier = jnp.where(across_at < down_at, 1.0, 0.0).astype(BF16)
    before = dot(earlier, (match0 + match1).astype(BF16))
    place0 = first * cap + jnp.sum(before * match0, axis=1, keepdims=True)
    place1 = second * cap + jnp.sum(before * match1, axis=1, keepdims=True)
    slot = lax.broadcasted_iota(jnp.int32, (rows, slots), 1).astype(F32)
    pick0 = jnp.where(slot == place0, 1.0, 0.0)
    pick1 = jnp.where(slot == place1, 1.0, 0.0)
    pick[0:rows, :] = pick0.astype(BF16)
    pick[rows : 2 * rows, :] = pick1.astype(BF16)
    either = (pick0 + pick1).astype(BF16)
    for copy in loads[4:]:
        copy.wait()
    pl.semaphore_wait(barrier, near + n_tp - 1)

    for n in range(3):
        target = second_set[n].at[tp]
        remote(slices[n], target, relay_send, relay_recv.at[n], (other, tp)).start()
    for n in range(3):
        ring_step(0, shared_set, n, 0)

    swap[...] = order_matrix(TILE, TILE)
    swap_out[...] = order_matrix(TILE, half_blocks)
    swap_in[...] = order_matrix(half_blocks, TILE)

    wide = 2 * LANES
    for j in range(width // wide):
        columns = pl.ds(j * wide, wide)
        flat[:, columns] = lax.dot_general(
            either, normed[:, columns], (((0,), (0,)), ((), ())), preferred_element_type=F32
        ).astype(BF16)

    def pack(i, carry):
        for u in range(unroll):
            at = pl.ds(pl.multiple_of((i * unroll + u) * TILE, TILE), TILE)
            mixed = swapped(
                swap[...], lambda b, at=at: flat[at, pl.ds(b * LANES, LANES)], blocks
            )
            outgoing[at] = mixed.reshape(TILE, TILE, LANES)
        return carry

    lax.fori_loop(0, slots // TILE // unroll, pack, 0)

    def send_home(place, carry):
        to_z, to_x = partner(place, 0, 1)
        target = to_z * N_X + to_x

        @pl.when(place != own)
        def _():
            remote(
                outgoing.at[pl.ds(target * cap, cap)], arrived.at[pl.ds(place * cap, cap)],
                send_sem, arrive_sem.at[place // chunk], (target, tp),
            ).start()

        return carry

    def send_second(place, carry):
        to_z, to_x = partner(place, 1, 1)
        target = to_z * N_X + to_x
        served = lax.rem(target + n_ep // 2, n_ep)
        there = places + place

        @pl.when(place != own)
        def _():
            remote(
                outgoing.at[pl.ds(served * cap, cap)], arrived.at[pl.ds(there * cap, cap)],
                send_sem, arrive_sem.at[there // chunk], (target, tp),
            ).start()

        return carry

    lax.fori_loop(own + 1, places, send_home, 0)
    lax.fori_loop(own + 1, places, send_second, 0)
    arrived[pl.ds(own * cap, cap)] = outgoing[pl.ds(me * cap, cap)]
    arrived[pl.ds((places + own) * cap, cap)] = outgoing[pl.ds(other * cap, cap)]

    def expert_step(n, weights):
        gate_ref, up_ref, down_ref = weights
        base = n * span
        full = n * chunk // places * places + own < n * chunk or (
            n * chunk // places * places + own >= (n + 1) * chunk
        )
        awaited = arrived.at[pl.ds(base, span if full else span - cap)]
        remote(awaited, awaited, send_sem, arrive_sem.at[n], (me, tp)).wait_recv()
        for g in range(span // TILE):
            at = pl.ds(g * TILE, TILE)
            mixed = swapped(swap[...], lambda b, g=g: arrived[base + g * TILE + b], TILE)
            for b in range(blocks):
                xs[at, pl.ds(b * LANES, LANES)] = mixed[TILE * b : TILE * (b + 1), :]
        taken = xs[...]
        ff = gate_ref.shape[2]
        gate = dot(taken, gate_ref[...].reshape(width, ff))
        hidden = silu_mul(gate, dot(taken, up_ref[...].reshape(width, ff)))
        for j in range(width // 512):
            columns = pl.ds(j * 512, 512)
            rs[:, columns] = dot(hidden, down_ref[:, :, columns].reshape(ff, 512)).astype(BF16)
        for h in range(2):
            for g in range(span // TILE):
                at = pl.ds(g * TILE, TILE)
                mixed = swapped(
                    swap_out[...],
                    lambda b, at=at, h=h: rs[at, pl.ds((2 * b + h) * LANES, LANES)],
                    half_blocks,
                )
                results[h, pl.ds(base // 2 + g * half_blocks, half_blocks)] = mixed.reshape(
                    half_blocks, TILE, LANES
                )

    def send_back(half, start, stop, odd):
        base = odd * places
        served = other if odd else me

        def one(place, carry):
            to_z, to_x = partner(place, odd, -1)

            @pl.when(place != own)
            def _():
                remote(
                    results.at[half, pl.ds((base + place) * half_cap, half_cap)],
                    returned.at[half, pl.ds(served * half_cap, half_cap)],
                    back_send.at[half], back_recv.at[half], (to_z * N_X + to_x, tp),
                ).start()

            return carry

        lax.fori_loop(start, stop, one, 0)

    def keep_own(odd):
        served = other if odd else me
        for h in range(2):
            returned[h, pl.ds(served * half_cap, half_cap)] = results[
                h, pl.ds((odd * places + own) * half_cap, half_cap)
            ]

    order = sorted((2 * n + step, n, step) for n in range(3) for step in range(ahead + 1))
    for _, n, step in order:
        if step == 0:
            block = second_set[n].at[tp]
            remote(block, block, relay_send, relay_recv.at[n], (me, tp)).wait_recv()
        ring_step(1, second_set, n, step)
        if (n, step) == (2, 0):
            lax.fori_loop(0, own, send_home, 0)
            lax.fori_loop(0, own, send_second, 0)

    for copy in weight_copies:
        copy.wait()
    for n in range(2 * n_chunks):
        if n == n_chunks:
            keep_own(0)
            ring_end(1, second_set)
        if n % 2 == 0 and 1 + n // 2 < ahead:
            for part in range(3):
                ring_step(0, shared_set, part, 1 + n // 2)
        expert_step(n, first_set if n < n_chunks else second_set)
        odd = n // n_chunks
        begin = n % n_chunks * chunk
        send_back(0, begin, begin + chunk, odd)
    keep_own(1)
    send_back(1, 0, places, 0)
    send_back(1, 0, places, 1)

    for n in range(3):
        ring_step(0, shared_set, n, ahead)
    ring_end(0, shared_set)
    sh_ff = all_gate.shape[2]
    gate_sum = dot(normed[...], all_gate[...].reshape(width, sh_ff))
    up_sum = dot(normed[...], all_up[...].reshape(width, sh_ff))
    shared_hidden = silu_mul(gate_sum, up_sum)
    out_width = width // n_tp
    for t in range(0, n_tp, 2):
        both = jnp.concatenate([all_down[t], all_down[t + 1]], axis=1)
        shared[:, pl.ds(t * out_width, 2 * out_width)] = dot(shared_hidden, both).astype(BF16)

    weight0, weight1 = column(gates[0:1, :]), column(gates[1:2, :])
    squares = jnp.zeros((rows, LANES), F32)
    for h in range(2):
        rest = pl.ds(0, (n_ep - 2) * half_cap)
        remote(
            results.at[h, rest], returned.at[h, rest], back_send.at[h], back_recv.at[h], (me, tp)
        ).wait_recv()

        def unpack(i, carry, h=h):
            for u in range(unroll):
                group = i * unroll + u
                tile = group * half_blocks
                mixed = swapped(
                    swap_in[...], lambda b, tile=tile: returned[h, tile + b], half_blocks
                )
                at = pl.ds(pl.multiple_of(group * TILE, TILE), TILE)
                for b in range(half_blocks):
                    half_flat[at, pl.ds(b * LANES, LANES)] = mixed[TILE * b : TILE * (b + 1), :]
            return carry

        lax.fori_loop(0, slots // TILE // unroll, unpack, 0)
        for jj in range(half_blocks // 2):
            picked = dot(pick[...], half_flat[:, pl.ds(jj * wide, wide)])
            routed = (weight0 * picked[0:rows] + weight1 * picked[rows : 2 * rows]).astype(BF16)
            for b in range(2):
                block = 2 * (2 * jj + b) + h
                total = routed[:, b * LANES : (b + 1) * LANES].astype(F32) + shared[
                    :, pl.ds(block * LANES, LANES)
                ].astype(F32)
                squares += total * total
                per = out_width // LANES
                out_blocks[block // per, :, pl.ds(block % per * LANES, LANES)] = total.astype(BF16)
        if out_width == LANES:
            send_out(h, n_row, row, tp, me, remote, out_blocks, out_landed, out_send, out_recv)
    if out_width != LANES:
        for h in range(2):
            send_out(h, n_row, row, tp, me, remote, out_blocks, out_landed, out_send, out_recv)

    scale_out = lax.rsqrt(jnp.sum(squares, axis=1, keepdims=True) * (1.0 / width) + 1e-06)
    scale_line = jnp.sum(jnp.where(diagonal, scale_out, 0.0), axis=0, keepdims=True)
    scales[...] = jnp.broadcast_to(scale_line, scales.shape)

    def send_scale(i, carry):
        target = lax.rem(tp + i, n_tp)
        remote(scales, scales_landed.at[tp], scale_send, scale_recv, (me, target)).start()
        return carry

    lax.fori_loop(1, n_tp, send_scale, 0)
    out_landed[tp] = out_blocks[tp]
    scales_landed[tp] = scales[...]

    three = wg2.at[pl.ds(0, 3)]
    remote(three, three, relay_send, relay_recv.at[0], (me, tp)).wait_send()
    rest = pl.ds(0, (n_ep - 2) * cap)
    remote(outgoing.at[rest], arrived.at[rest], send_sem, arrive_sem.at[0], (me, tp)).wait_send()
    for h in range(2):
        rest = pl.ds(0, (n_ep - 2) * half_cap)
        remote(
            results.at[h, rest], returned.at[h, rest], back_send.at[h], back_recv.at[h], (me, tp)
        ).wait_send()
    others = pl.ds(0, n_tp - 1)
    some = scales_landed.at[others]
    remote(some, some, scale_send, scale_recv, (me, tp)).wait()
    some = out_landed.at[others]
    remote(some, some, out_send, out_recv, (me, tp)).wait()


def finish(landed, scales, post_gain, out):
    sources, rows, out_width = landed.shape
    at = pl.multiple_of(lax.axis_index("tp") * out_width, LANES)
    gain = post_gain[:, pl.ds(at, out_width)]
    down_at = lax.broadcasted_iota(jnp.int32, (rows, rows), 0)
    diagonal = down_at == lax.broadcasted_iota(jnp.int32, (rows, rows), 1)
    for t in range(sources):
        scale = jnp.sum(jnp.where(diagonal, scales[t, 0:1, :], 0.0), axis=1, keepdims=True)
        out[t] = (landed[t].astype(F32) * scale * gain).astype(BF16)


def send_out(h, n_row, row, tp, me, remote, out_blocks, out_landed, out_send, out_recv):
    def one(i, carry):
        target = 2 * lax.rem(row + i, n_row) + h

        @pl.when(target != tp)
        def _():
            remote(
                out_blocks.at[target], out_landed.at[tp], out_send, out_recv, (me, target)
            ).start()

        return carry

    lax.fori_loop(0, n_row, one, 0)


def per_device(
    tokens, routes, gates, pre_gain, w_gate, w_up, w_down, sh_gate, sh_up, sh_down, post_gain
):
    rows, width = tokens.shape
    n_ep, n_tp = lax.axis_size("ep"), lax.axis_size("tp")
    ff = w_gate.shape[2]
    cap = max(2, 4 * rows * TOPK // (3 * n_ep))
    chunk = 8
    slots = n_ep * cap
    n_row = n_tp // 2
    depth, sh_ff = sh_gate.shape
    out_width = width // n_tp
    half_blocks = width // LANES // 2
    vmem = pl.BlockSpec(memory_space=pltpu.VMEM)
    anywhere = pl.BlockSpec(memory_space=pl.ANY)
    dma = pltpu.SemaphoreType.DMA
    tiles = pltpu.VMEM((slots, TILE, LANES), BF16)
    halves = pltpu.VMEM((2, slots // 2, TILE, LANES), BF16)
    in_rows = pltpu.VMEM((n_tp, width // n_tp, ff), BF16)
    out_rows = pltpu.VMEM((n_tp, ff // n_tp, width), BF16)
    landed, scales = pl.pallas_call(
        functools.partial(kernel, n_ep, n_tp, cap, chunk),
        out_shape=(
            jax.ShapeDtypeStruct((n_tp, rows, out_width), BF16),
            jax.ShapeDtypeStruct((n_tp, 8, rows), F32),
        ),
        in_specs=[anywhere] * 10,
        out_specs=(vmem, vmem),
        scratch_shapes=[
            pltpu.VMEM((rows, width), BF16),
            pltpu.VMEM((2, rows), jnp.int32),
            pltpu.VMEM((2, rows), F32),
            pltpu.VMEM((1, width), F32),
            pltpu.VMEM((width // n_tp, ff), BF16),
            pltpu.VMEM((width // n_tp, ff), BF16),
            pltpu.VMEM((ff // n_tp, width), BF16),
            pltpu.VMEM((rows, width), BF16),
            pltpu.VMEM((2 * rows, slots), BF16),
            pltpu.VMEM((TILE * TILE, TILE * TILE), BF16),
            pltpu.VMEM((TILE * half_blocks, TILE * half_blocks), BF16),
            pltpu.VMEM((TILE * half_blocks, TILE * half_blocks), BF16),
            pltpu.VMEM((slots, width), BF16),
            pltpu.VMEM((slots, width // 2), BF16),
            tiles, tiles, halves, halves,
            in_rows, in_rows, out_rows, in_rows, in_rows, out_rows,
            pltpu.VMEM((chunk * cap, width), BF16),
            pltpu.VMEM((chunk * cap, width), BF16),
            pltpu.VMEM((n_tp, depth, sh_ff), BF16),
            pltpu.VMEM((n_tp, depth, sh_ff), BF16),
            pltpu.VMEM((n_tp, sh_ff, out_width), BF16),
            pltpu.VMEM((rows, width), BF16),
            pltpu.VMEM((n_tp, rows, out_width), BF16),
            pltpu.VMEM((8, rows), F32),
            dma((10,)), dma((3,)), dma, dma((3,)), dma, dma((n_ep // chunk,)), dma((2,)), dma((2,)),
            dma((2, 2)), dma((6, 2, n_row // 2)), dma((2, 3)), dma((2, 3)),
            dma, dma, dma, dma,
        ],
        compiler_params=pltpu.CompilerParams(
            collective_id=0, has_side_effects=True, vmem_limit_bytes=60 * 1024 * 1024
        ),
    )(
        tokens, routes.T, gates.T, pre_gain.reshape(1, width),
        w_gate.reshape(n_tp, width // n_tp, ff), w_up.reshape(n_tp, width // n_tp, ff),
        w_down.reshape(n_tp, ff // n_tp, width),
        sh_gate, sh_up, sh_down,
    )
    some = n_tp // 4
    result = pl.pallas_call(
        finish,
        grid=(4,),
        out_shape=jax.ShapeDtypeStruct((n_tp, rows, out_width), BF16),
        in_specs=[
            pl.BlockSpec((some, rows, out_width), lambda i: (i, 0, 0)),
            pl.BlockSpec((some, 8, rows), lambda i: (i, 0, 0)),
            pl.BlockSpec((1, width), lambda i: (0, 0)),
        ],
        out_specs=pl.BlockSpec((some, rows, out_width), lambda i: (i, 0, 0)),
    )(landed, scales, post_gain.reshape(1, width))
    return result.reshape(n_tp * rows, out_width)


def solution(mesh):
    return jax.shard_map(
        per_device,
        mesh=mesh,
        in_specs=(
            P(("ep", "tp"), None),
            P(("ep", "tp"), None),
            P(("ep", "tp"), None),
            P(),
            P("ep", None, None),
            P("ep", None, None),
            P("ep", None, None),
            P("tp", None),
            P("tp", None),
            P(None, "tp"),
            P(),
        ),
        out_specs=P("ep", "tp"),
        check_vma=False,
    )
```

```python
import functools

import jax
import jax.numpy as jnp
from jax import lax
from jax.experimental import pallas as pl
from jax.experimental.pallas import tpu as pltpu
from jax.sharding import PartitionSpec as P

TOPK = 2
LANES = 128
TILE = 16
N_X = 4
MESH = pl.DeviceIdType.MESH
F32 = jnp.float32
BF16 = jnp.bfloat16


def dot(a, b):
    return jnp.dot(a, b, preferred_element_type=F32)


def silu_mul(gate, up):
    return (gate / (1.0 + jnp.exp(-gate)) * up).astype(BF16)


def offset_at(place, reach, odd):
    groups = 2 * reach
    group, item = place // 4, lax.rem(place, 4)
    first = 1 - (group + groups - 2) // (groups - 1)
    later = group - 1 + first
    ring = first * reach * (1 - 2 * lax.rem(item, 2)) + (1 - first) * (
        (reach - 1 - later // 2) * (1 - 2 * lax.rem(later, 2))
    )
    return ring, first * (2 * (item // 2) + odd) + (1 - first) * item


def swapped(swap, read, blocks):
    stacked = jnp.concatenate([read(b) for b in range(blocks)], axis=0)
    return dot(swap, stacked).astype(BF16)


def order_matrix(outer, inner):
    side = outer * inner
    to = lax.broadcasted_iota(jnp.int32, (side, side), 0)
    come = lax.broadcasted_iota(jnp.int32, (side, side), 1)
    return jnp.where(come == lax.rem(to, inner) * outer + to // inner, 1.0, 0.0).astype(BF16)


def kernel(
    n_ep, n_tp, cap, chunk,
    tokens_in, routes_in, gates_in, pre_gain_in, w_gate, w_up, w_down, sh_gate, sh_up, sh_down,
    out_landed, scales_landed,
    tokens, routes, gates, pre_gain, slice_gate, slice_up, slice_down,
    normed, pick, swap, swap_out, swap_in, flat, half_flat, outgoing, arrived, results, returned,
    wg, wu, wd, wg2, wu2, wd2, xs, rs, all_gate, all_up, all_down, shared,
    out_blocks, scales,
    in_sem, w_sem, relay_send, relay_recv, send_sem, arrive_sem, back_send, back_recv,
    ring_send, ring_recv, pair_send, pair_recv,
    out_send, out_recv, scale_send, scale_recv,
):
    me, tp = lax.axis_index("ep"), lax.axis_index("tp")
    core, row = lax.rem(tp, 2), tp // 2
    n_row = n_tp // 2
    n_z = n_ep // N_X
    reach = n_z // 4
    z, x = me // N_X, lax.rem(me, N_X)
    rows, width = tokens.shape
    slots = n_ep * cap
    unroll = next(u for u in (5, 4, 3, 2, 1) if slots // TILE % u == 0)
    places = n_ep // 2
    n_chunks = places // chunk
    span = chunk * cap
    own = places - 4
    blocks = width // LANES
    half_blocks = blocks // 2
    half_cap = cap // 2
    other = lax.rem(me + n_ep // 2, n_ep)
    pair = tp + 1 - 2 * core

    def partner(place, odd, sign):
        ring, side = offset_at(place, reach, odd)
        return lax.rem(z + n_z + sign * ring, n_z), lax.rem(x + N_X + sign * side, N_X)

    def remote(source, target, send, receive, device):
        return pltpu.make_async_remote_copy(
            src_ref=source, dst_ref=target, send_sem=send, recv_sem=receive,
            device_id=device, device_id_type=MESH,
        )

    barrier = pltpu.get_barrier_semaphore()

    near = (2 * reach + 1) * N_X
    itself = reach * N_X

    def greet_near(i, carry):
        at_z = lax.rem(z + n_z + i // N_X - reach, n_z)
        device = (at_z * N_X + lax.rem(x + lax.rem(i, N_X), N_X), tp)
        pl.semaphore_signal(barrier, inc=1, device_id=device, device_id_type=MESH)
        return carry

    def greet_tp(i, carry):
        device = (me, lax.rem(tp + i, n_tp))
        pl.semaphore_signal(barrier, inc=1, device_id=device, device_id_type=MESH)
        return carry

    first_set = (wg, wu, wd)
    second_set = (wg2, wu2, wd2)
    shared_set = (all_gate, all_up, all_down)
    slices = (slice_gate, slice_up, slice_down)
    loads = [
        pltpu.make_async_copy(source, target, in_sem.at[i])
        for i, (source, target) in enumerate(
            (
                (tokens_in, tokens), (pre_gain_in, pre_gain), (routes_in, routes),
                (gates_in, gates),
                (w_gate.at[tp], slice_gate), (w_up.at[tp], slice_up), (w_down.at[tp], slice_down),
                (sh_gate, all_gate.at[tp]), (sh_up, all_up.at[tp]), (sh_down, all_down.at[tp]),
            )
        )
    ]
    for copy in loads:
        copy.start()
    pl.semaphore_signal(barrier, inc=1, device_id=(other, tp), device_id_type=MESH)
    lax.fori_loop(0, itself, greet_near, 0)
    lax.fori_loop(itself + 1, near, greet_near, 0)
    lax.fori_loop(1, n_tp, greet_tp, 0)
    weight_copies = [
        pltpu.make_async_copy(source, target, w_sem.at[i])
        for i, (source, target) in enumerate(zip((w_gate, w_up, w_down), first_set))
    ]
    for copy in weight_copies:
        copy.start()
    for copy in loads[:4]:
        copy.wait()

    ahead = n_row // 2
    behind = n_row - 1 - ahead
    up_row = 2 * lax.rem(row + 1, n_row) + core
    down_row = 2 * lax.rem(row + n_row - 1, n_row) + core

    def ring_step(k, whole, n, step):
        ref = whole[n]
        ups, downs = (ahead, behind) if n < 2 else (behind, ahead)
        below = ref.at[2 * lax.rem(row + n_row - step, n_row) + core]
        above = ref.at[2 * lax.rem(row + step, n_row) + core]
        ways = ((0, below, ups, up_row), (1, above, downs, down_row))
        for way, block, hops, _ in ways:
            if 1 <= step <= hops:
                receive = ring_recv.at[3 * k + n, way, step - 1]
                remote(block, block, ring_send.at[k, way], receive, (me, tp)).wait_recv()
        for way, block, hops, target in ways:
            if step < hops:
                receive = ring_recv.at[3 * k + n, way, step]
                remote(block, block, ring_send.at[k, way], receive, (me, target)).start()
        for way, block, hops, _ in ways:
            if way <= step <= hops:
                remote(block, block, pair_send.at[k, n], pair_recv.at[k, n], (me, pair)).start()

    def ring_end(k, whole):
        for n, ref in enumerate(whole):
            part = ref.at[pl.ds(0, n_row)]
            remote(part, part, pair_send.at[k, n], pair_recv.at[k, n], (me, tp)).wait()
        for way, count in ((0, 2 * ahead + behind), (1, 2 * behind + ahead)):
            part = whole[0].at[pl.ds(0, count)]
            receive = ring_recv.at[3 * k, way, 0]
            remote(part, part, ring_send.at[k, way], receive, (me, tp)).wait_send()

    def norm_rows(i, carry):
        at = pl.ds(pl.multiple_of(i * 3 * TILE, TILE), 3 * TILE)
        values = tokens[at, :].astype(F32)
        scale = lax.rsqrt(jnp.mean(values * values, axis=1, keepdims=True) + 1e-06)
        normed[at, :] = (values * scale * pre_gain[...]).astype(BF16)
        return carry

    lax.fori_loop(0, rows // (3 * TILE), norm_rows, 0)

    down_at = lax.broadcasted_iota(jnp.int32, (rows, rows), 0)
    across_at = lax.broadcasted_iota(jnp.int32, (rows, rows), 1)
    diagonal = down_at == across_at

    def column(values):
        return jnp.sum(jnp.where(diagonal, values, 0.0), axis=1, keepdims=True)

    expert = lax.broadcasted_iota(jnp.int32, (rows, LANES), 1).astype(F32)
    first = column(routes[0:1, :].astype(F32))
    second = column(routes[1:2, :].astype(F32))
    match0 = jnp.where(first == expert, 1.0, 0.0)
    match1 = jnp.where(second == expert, 1.0, 0.0)
    earlier = jnp.where(across_at < down_at, 1.0, 0.0).astype(BF16)
    before = dot(earlier, (match0 + match1).astype(BF16))
    place0 = first * cap + jnp.sum(before * match0, axis=1, keepdims=True)
    place1 = second * cap + jnp.sum(before * match1, axis=1, keepdims=True)
    slot = lax.broadcasted_iota(jnp.int32, (rows, slots), 1).astype(F32)
    pick0 = jnp.where(slot == place0, 1.0, 0.0)
    pick1 = jnp.where(slot == place1, 1.0, 0.0)
    pick[0:rows, :] = pick0.astype(BF16)
    pick[rows : 2 * rows, :] = pick1.astype(BF16)
    either = (pick0 + pick1).astype(BF16)
    for copy in loads[4:]:
        copy.wait()
    pl.semaphore_wait(barrier, near + n_tp - 1)

    for n in range(3):
        target = second_set[n].at[tp]
        remote(slices[n], target, relay_send, relay_recv.at[n], (other, tp)).start()
    for n in range(3):
        ring_step(0, shared_set, n, 0)

    swap[...] = order_matrix(TILE, TILE)
    swap_out[...] = order_matrix(TILE, half_blocks)
    swap_in[...] = order_matrix(half_blocks, TILE)

    wide = 2 * LANES
    for j in range(width // wide):
        columns = pl.ds(j * wide, wide)
        flat[:, columns] = lax.dot_general(
            either, normed[:, columns], (((0,), (0,)), ((), ())), preferred_element_type=F32
        ).astype(BF16)

    def pack(i, carry):
        for u in range(unroll):
            at = pl.ds(pl.multiple_of((i * unroll + u) * TILE, TILE), TILE)
            mixed = swapped(
                swap[...], lambda b, at=at: flat[at, pl.ds(b * LANES, LANES)], blocks
            )
            outgoing[at] = mixed.reshape(TILE, TILE, LANES)
        return carry

    lax.fori_loop(0, slots // TILE // unroll, pack, 0)

    def send_home(place, carry):
        to_z, to_x = partner(place, 0, 1)
        target = to_z * N_X + to_x

        @pl.when(place != own)
        def _():
            remote(
                outgoing.at[pl.ds(target * cap, cap)], arrived.at[pl.ds(place * cap, cap)],
                send_sem, arrive_sem.at[place // chunk], (target, tp),
            ).start()

        return carry

    def send_second(place, carry):
        to_z, to_x = partner(place, 1, 1)
        target = to_z * N_X + to_x
        served = lax.rem(target + n_ep // 2, n_ep)
        there = places + place

        @pl.when(place != own)
        def _():
            remote(
                outgoing.at[pl.ds(served * cap, cap)], arrived.at[pl.ds(there * cap, cap)],
                send_sem, arrive_sem.at[there // chunk], (target, tp),
            ).start()

        return carry

    lax.fori_loop(0, places, send_home, 0)
    lax.fori_loop(0, places, send_second, 0)
    arrived[pl.ds(own * cap, cap)] = outgoing[pl.ds(me * cap, cap)]
    arrived[pl.ds((places + own) * cap, cap)] = outgoing[pl.ds(other * cap, cap)]

    def expert_step(n, weights):
        gate_ref, up_ref, down_ref = weights
        base = n * span
        full = n * chunk // places * places + own < n * chunk or (
            n * chunk // places * places + own >= (n + 1) * chunk
        )
        awaited = arrived.at[pl.ds(base, span if full else span - cap)]
        remote(awaited, awaited, send_sem, arrive_sem.at[n], (me, tp)).wait_recv()
        for g in range(span // TILE):
            at = pl.ds(g * TILE, TILE)
            mixed = swapped(swap[...], lambda b, g=g: arrived[base + g * TILE + b], TILE)
            for b in range(blocks):
                xs[at, pl.ds(b * LANES, LANES)] = mixed[TILE * b : TILE * (b + 1), :]
        taken = xs[...]
        ff = gate_ref.shape[2]
        gate = dot(taken, gate_ref[...].reshape(width, ff))
        hidden = silu_mul(gate, dot(taken, up_ref[...].reshape(width, ff)))
        for j in range(width // 512):
            columns = pl.ds(j * 512, 512)
            rs[:, columns] = dot(hidden, down_ref[:, :, columns].reshape(ff, 512)).astype(BF16)
        for h in range(2):
            for g in range(span // TILE):
                at = pl.ds(g * TILE, TILE)
                mixed = swapped(
                    swap_out[...],
                    lambda b, at=at, h=h: rs[at, pl.ds((2 * b + h) * LANES, LANES)],
                    half_blocks,
                )
                results[h, pl.ds(base // 2 + g * half_blocks, half_blocks)] = mixed.reshape(
                    half_blocks, TILE, LANES
                )

    def send_back(half, start, stop, odd):
        base = odd * places
        served = other if odd else me

        def one(place, carry):
            to_z, to_x = partner(place, odd, -1)

            @pl.when(place != own)
            def _():
                remote(
                    results.at[half, pl.ds((base + place) * half_cap, half_cap)],
                    returned.at[half, pl.ds(served * half_cap, half_cap)],
                    back_send.at[half], back_recv.at[half], (to_z * N_X + to_x, tp),
                ).start()

            return carry

        lax.fori_loop(start, stop, one, 0)

    def keep_own(odd):
        served = other if odd else me
        for h in range(2):
            returned[h, pl.ds(served * half_cap, half_cap)] = results[
                h, pl.ds((odd * places + own) * half_cap, half_cap)
            ]

    between = {(0, 0): 1, (1, 3): 2}
    order = sorted((2 * n + step, n, step) for n in range(3) for step in range(ahead + 1))
    for _, n, step in order:
        if step == 0:
            block = second_set[n].at[tp]
            remote(block, block, relay_send, relay_recv.at[n], (me, tp)).wait_recv()
        ring_step(1, second_set, n, step)
        if (n, step) in between and between[n, step] < ahead:
            for part in range(3):
                ring_step(0, shared_set, part, between[n, step])

    for copy in weight_copies:
        copy.wait()
    for n in range(2 * n_chunks):
        if n == n_chunks:
            keep_own(0)
            ring_end(1, second_set)
        if n == 2 and ahead > 3:
            for part in range(3):
                ring_step(0, shared_set, part, 3)
        expert_step(n, first_set if n < n_chunks else second_set)
        odd = n // n_chunks
        begin = n % n_chunks * chunk
        send_back(0, begin, begin + chunk, odd)
        if n == n_chunks:
            send_back(1, 0, places, 0)
    keep_own(1)
    send_back(1, 0, places, 1)

    for n in range(3):
        ring_step(0, shared_set, n, ahead)
    ring_end(0, shared_set)
    sh_ff = all_gate.shape[2]
    gate_sum = dot(normed[...], all_gate[...].reshape(width, sh_ff))
    up_sum = dot(normed[...], all_up[...].reshape(width, sh_ff))
    shared_hidden = silu_mul(gate_sum, up_sum)
    out_width = width // n_tp
    for t in range(0, n_tp, 2):
        both = jnp.concatenate([all_down[t], all_down[t + 1]], axis=1)
        shared[:, pl.ds(t * out_width, 2 * out_width)] = dot(shared_hidden, both).astype(BF16)

    weight0, weight1 = column(gates[0:1, :]), column(gates[1:2, :])
    squares = jnp.zeros((rows, LANES), F32)
    for h in range(2):
        rest = pl.ds(0, (n_ep - 2) * half_cap)
        remote(
            results.at[h, rest], returned.at[h, rest], back_send.at[h], back_recv.at[h], (me, tp)
        ).wait_recv()

        def unpack(i, carry, h=h):
            for u in range(unroll):
                group = i * unroll + u
                tile = group * half_blocks
                mixed = swapped(
                    swap_in[...], lambda b, tile=tile: returned[h, tile + b], half_blocks
                )
                at = pl.ds(pl.multiple_of(group * TILE, TILE), TILE)
                for b in range(half_blocks):
                    half_flat[at, pl.ds(b * LANES, LANES)] = mixed[TILE * b : TILE * (b + 1), :]
            return carry

        lax.fori_loop(0, slots // TILE // unroll, unpack, 0)
        for jj in range(half_blocks // 2):
            picked = dot(pick[...], half_flat[:, pl.ds(jj * wide, wide)])
            routed = (weight0 * picked[0:rows] + weight1 * picked[rows : 2 * rows]).astype(BF16)
            for b in range(2):
                block = 2 * (2 * jj + b) + h
                total = routed[:, b * LANES : (b + 1) * LANES].astype(F32) + shared[
                    :, pl.ds(block * LANES, LANES)
                ].astype(F32)
                squares += total * total
                per = out_width // LANES
                out_blocks[block // per, :, pl.ds(block % per * LANES, LANES)] = total.astype(BF16)
        if out_width == LANES:
            send_out(h, n_row, row, tp, me, remote, out_blocks, out_landed, out_send, out_recv)
    if out_width != LANES:
        for h in range(2):
            send_out(h, n_row, row, tp, me, remote, out_blocks, out_landed, out_send, out_recv)

    scale_out = lax.rsqrt(jnp.sum(squares, axis=1, keepdims=True) * (1.0 / width) + 1e-06)
    scale_line = jnp.sum(jnp.where(diagonal, scale_out, 0.0), axis=0, keepdims=True)
    scales[...] = jnp.broadcast_to(scale_line, scales.shape)

    def send_scale(i, carry):
        target = lax.rem(tp + i, n_tp)
        remote(scales, scales_landed.at[tp], scale_send, scale_recv, (me, target)).start()
        return carry

    lax.fori_loop(1, n_tp, send_scale, 0)
    out_landed[tp] = out_blocks[tp]
    scales_landed[tp] = scales[...]

    three = wg2.at[pl.ds(0, 3)]
    remote(three, three, relay_send, relay_recv.at[0], (me, tp)).wait_send()
    rest = pl.ds(0, (n_ep - 2) * cap)
    remote(outgoing.at[rest], arrived.at[rest], send_sem, arrive_sem.at[0], (me, tp)).wait_send()
    for h in range(2):
        rest = pl.ds(0, (n_ep - 2) * half_cap)
        remote(
            results.at[h, rest], returned.at[h, rest], back_send.at[h], back_recv.at[h], (me, tp)
        ).wait_send()
    others = pl.ds(0, n_tp - 1)
    some = scales_landed.at[others]
    remote(some, some, scale_send, scale_recv, (me, tp)).wait()
    some = out_landed.at[others]
    remote(some, some, out_send, out_recv, (me, tp)).wait()


def finish(landed, scales, post_gain, out):
    sources, rows, out_width = landed.shape
    at = pl.multiple_of(lax.axis_index("tp") * out_width, LANES)
    gain = post_gain[:, pl.ds(at, out_width)]
    down_at = lax.broadcasted_iota(jnp.int32, (rows, rows), 0)
    diagonal = down_at == lax.broadcasted_iota(jnp.int32, (rows, rows), 1)
    for t in range(sources):
        scale = jnp.sum(jnp.where(diagonal, scales[t, 0:1, :], 0.0), axis=1, keepdims=True)
        out[t] = (landed[t].astype(F32) * scale * gain).astype(BF16)


def send_out(h, n_row, row, tp, me, remote, out_blocks, out_landed, out_send, out_recv):
    def one(i, carry):
        target = 2 * lax.rem(row + i, n_row) + h

        @pl.when(target != tp)
        def _():
            remote(
                out_blocks.at[target], out_landed.at[tp], out_send, out_recv, (me, target)
            ).start()

        return carry

    lax.fori_loop(0, n_row, one, 0)


def per_device(
    tokens, routes, gates, pre_gain, w_gate, w_up, w_down, sh_gate, sh_up, sh_down, post_gain
):
    rows, width = tokens.shape
    n_ep, n_tp = lax.axis_size("ep"), lax.axis_size("tp")
    ff = w_gate.shape[2]
    cap = max(2, 4 * rows * TOPK // (3 * n_ep))
    chunk = 8
    slots = n_ep * cap
    n_row = n_tp // 2
    depth, sh_ff = sh_gate.shape
    out_width = width // n_tp
    half_blocks = width // LANES // 2
    vmem = pl.BlockSpec(memory_space=pltpu.VMEM)
    anywhere = pl.BlockSpec(memory_space=pl.ANY)
    dma = pltpu.SemaphoreType.DMA
    tiles = pltpu.VMEM((slots, TILE, LANES), BF16)
    halves = pltpu.VMEM((2, slots // 2, TILE, LANES), BF16)
    in_rows = pltpu.VMEM((n_tp, width // n_tp, ff), BF16)
    out_rows = pltpu.VMEM((n_tp, ff // n_tp, width), BF16)
    landed, scales = pl.pallas_call(
        functools.partial(kernel, n_ep, n_tp, cap, chunk),
        out_shape=(
            jax.ShapeDtypeStruct((n_tp, rows, out_width), BF16),
            jax.ShapeDtypeStruct((n_tp, 8, rows), F32),
        ),
        in_specs=[anywhere] * 10,
        out_specs=(vmem, vmem),
        scratch_shapes=[
            pltpu.VMEM((rows, width), BF16),
            pltpu.VMEM((2, rows), jnp.int32),
            pltpu.VMEM((2, rows), F32),
            pltpu.VMEM((1, width), F32),
            pltpu.VMEM((width // n_tp, ff), BF16),
            pltpu.VMEM((width // n_tp, ff), BF16),
            pltpu.VMEM((ff // n_tp, width), BF16),
            pltpu.VMEM((rows, width), BF16),
            pltpu.VMEM((2 * rows, slots), BF16),
            pltpu.VMEM((TILE * TILE, TILE * TILE), BF16),
            pltpu.VMEM((TILE * half_blocks, TILE * half_blocks), BF16),
            pltpu.VMEM((TILE * half_blocks, TILE * half_blocks), BF16),
            pltpu.VMEM((slots, width), BF16),
            pltpu.VMEM((slots, width // 2), BF16),
            tiles, tiles, halves, halves,
            in_rows, in_rows, out_rows, in_rows, in_rows, out_rows,
            pltpu.VMEM((chunk * cap, width), BF16),
            pltpu.VMEM((chunk * cap, width), BF16),
            pltpu.VMEM((n_tp, depth, sh_ff), BF16),
            pltpu.VMEM((n_tp, depth, sh_ff), BF16),
            pltpu.VMEM((n_tp, sh_ff, out_width), BF16),
            pltpu.VMEM((rows, width), BF16),
            pltpu.VMEM((n_tp, rows, out_width), BF16),
            pltpu.VMEM((8, rows), F32),
            dma((10,)), dma((3,)), dma, dma((3,)), dma, dma((n_ep // chunk,)), dma((2,)), dma((2,)),
            dma((2, 2)), dma((6, 2, n_row // 2)), dma((2, 3)), dma((2, 3)),
            dma, dma, dma, dma,
        ],
        compiler_params=pltpu.CompilerParams(
            collective_id=0, has_side_effects=True, vmem_limit_bytes=60 * 1024 * 1024
        ),
    )(
        tokens, routes.T, gates.T, pre_gain.reshape(1, width),
        w_gate.reshape(n_tp, width // n_tp, ff), w_up.reshape(n_tp, width // n_tp, ff),
        w_down.reshape(n_tp, ff // n_tp, width),
        sh_gate, sh_up, sh_down,
    )
    some = n_tp // 4
    result = pl.pallas_call(
        finish,
        grid=(4,),
        out_shape=jax.ShapeDtypeStruct((n_tp, rows, out_width), BF16),
        in_specs=[
            pl.BlockSpec((some, rows, out_width), lambda i: (i, 0, 0)),
            pl.BlockSpec((some, 8, rows), lambda i: (i, 0, 0)),
            pl.BlockSpec((1, width), lambda i: (0, 0)),
        ],
        out_specs=pl.BlockSpec((some, rows, out_width), lambda i: (i, 0, 0)),
    )(landed, scales, post_gain.reshape(1, width))
    return result.reshape(n_tp * rows, out_width)


def solution(mesh):
    return jax.shard_map(
        per_device,
        mesh=mesh,
        in_specs=(
            P(("ep", "tp"), None),
            P(("ep", "tp"), None),
            P(("ep", "tp"), None),
            P(),
            P("ep", None, None),
            P("ep", None, None),
            P("ep", None, None),
            P("tp", None),
            P("tp", None),
            P(None, "tp"),
            P(),
        ),
        out_specs=P("ep", "tp"),
        check_vma=False,
    )
```
